32 devices in a mesh: sp: 8 (over z, core), tp: 4 (over y, x).
Axes of the slice: x: 2, y: 2, z: 4, core: 2. Of those that a mesh axis runs over, the one named last changes fastest.
Arguments:
- queries: bfloat16 [2048, 2048], P('sp', 'tp'), may hold values from -8 to 8
- key_rows: bfloat16 [2048, 1024], P('sp', 'tp'), may hold values from -8 to 8
- values: bfloat16 [2048, 1024], P('sp', 'tp'), may hold values from -6 to 6
- sink_logits: float32 [32], P('tp'), may hold values from 2 to 6
- residual: bfloat16 [2048, 2048], P(('sp', 'tp')), may hold values from -6 to 6
- out_weight: bfloat16 [2048, 2048], P('tp'), may hold values from -0.125 to 0.125
- norm_gain: float32 [2048], replicated, may hold values from 0.1 to 1.9
- expert_ids: int32 [2048, 2], P('sp'), may hold values from 0 to 7, as said below
- route_weight: float32 [2048, 2], P('sp'), may hold values from 0.2 to 1
- gate_proj: bfloat16 [8, 2048, 4096], P('sp', None, 'tp'), may hold values from -0.125 to 0.125
- up_proj: bfloat16 [8, 2048, 4096], P('sp', None, 'tp'), may hold values from -0.125 to 0.125
- down_proj: bfloat16 [8, 4096, 2048], P('sp', 'tp'), may hold values from -0.09375 to 0.09375
Outputs:
- mixed_out: bfloat16 [2048, 2048], P(('sp', 'tp'))
The draws below stay inside these ranges and needn't reach their ends.
Inputs may be any that keep to these rules, and one draw needn't show every extreme that they name: `expert_ids`: the two entries of a row are different experts of one group: experts g * 2 to g * 2 + 1 for a group g below 4. In each aligned block of 64 rows (the rows of one device) no expert is named more than 32 times, and one expert is named exactly 32 times in every block.
All inputs are finite; a program needn't handle non-finite values.
Results may differ from the reference program's by a relative error of at most 0.014.
Values may be sent and summed in bfloat16 or wider, within the bound.
A program may use at most 64 MiB of HBM per device.

```python
import math
import jax
import jax.numpy as jnp
from jax import lax

D = 2048
HEAD = 64
QH = 32
KVH = 16
WINDOW = 128
FFE = 4096
TOK_SP = 256
CAP = 32
SEQ = 2048
EXPERTS = 8
INNER = 2
N_SP = 8
N_TP = 4


def draw_queries(key, part):
    sampled = jnp.clip(jax.random.normal(jax.random.fold_in(key, 3), (SEQ, QH * HEAD), jnp.float32), -5.5, 5.5)
    return sampled.astype(jnp.bfloat16)


def draw_key_rows(key, part):
    sampled = jnp.clip(jax.random.normal(jax.random.fold_in(key, 8), (SEQ, KVH * HEAD), jnp.float32), -5.5, 5.5)
    return sampled.astype(jnp.bfloat16)


def draw_expert_ids(key, part):
    rows_per = TOK_SP // N_TP
    block_count = SEQ // rows_per
    favour = jax.random.randint(jax.random.fold_in(key, 5), (N_SP,), 0, 1500)
    jitter = jax.random.randint(jax.random.fold_in(key, 6), (block_count, rows_per, 2, N_SP), 0, 1000)
    forced = jax.random.randint(jax.random.fold_in(key, 7), (), 0, N_SP)
    labels = jnp.arange(N_SP, dtype=jnp.int32)
    family = labels // INNER
    same_family = (family[:, None] == family[None, :]).astype(jnp.int32)

    def one_block(block_jitter):

        def place(counts, entry_item):
            position, random_draws = entry_item
            has_room = (counts < CAP).astype(jnp.int32)
            family_room = jnp.sum(same_family * has_room[None, :], 1)
            usable = (has_room > 0) & (family_room >= 2)
            ranking = (random_draws[0] + favour) * N_SP + labels
            ranking = jnp.where((labels == forced) & (position < CAP), 100000000, ranking)
            ranking = jnp.where(usable, ranking, -1)
            first_pick = jnp.argmax(ranking).astype(jnp.int32)
            usable_two = (has_room > 0) & (family == family[first_pick]) & (labels != first_pick)
            ranking_two = jnp.where(usable_two, (random_draws[1] + favour) * N_SP + labels, -1)
            second = jnp.argmax(ranking_two).astype(jnp.int32)
            counts = counts + (labels == first_pick).astype(jnp.int32) + (labels == second).astype(jnp.int32)
            return (counts, jnp.stack([first_pick, second]))
        ignored, chosen = lax.scan(place, jnp.zeros((N_SP,), jnp.int32), (jnp.arange(rows_per, dtype=jnp.int32), block_jitter))
        return chosen
    return jax.vmap(one_block)(jitter).reshape(SEQ, 2).astype(jnp.int32)


def block_levels(key, dims, split, smallest, top_value):
    loudness, own = 1.0, jax.random.fold_in(key, 6)
    for axis_at, parts in split:
        draws = jnp.exp(jax.random.uniform(jax.random.fold_in(own, axis_at), (parts,), jnp.float32, smallest / len(split), top_value / len(split)))
        loudness = loudness * jnp.repeat(draws, dims[axis_at] // parts).reshape([-1 if axis == axis_at else 1 for axis in range(len(dims))])
    return loudness


def bell_draw(key, dims, spread, reach, pieces=(), kind=jnp.bfloat16):
    values = spread * jax.random.normal(key, dims, jnp.float32)
    if pieces:
        values = values * block_levels(key, dims, pieces, -0.22, 0.18)
    return jnp.clip(values, -reach, reach).astype(kind)


def setup_inputs(seed: int = 0) -> dict:
    splits = jax.random.split(jax.random.key(seed), 13)
    return {
        "queries": draw_queries(jax.random.fold_in(splits[12], 71), 0),
        "key_rows": draw_key_rows(jax.random.fold_in(splits[12], 71), 0),
        "values": bell_draw(splits[2], (SEQ, KVH * HEAD), 1.0, 6.0, ((0, 8), (1, 4))),
        "sink_logits": jnp.clip(2.0 + 4.0 * jax.random.uniform(splits[3], (QH,), jnp.float32) ** block_levels(splits[3], (QH,), ((0, 4),), -0.2, 0.2), 2.0, 6.0),
        "residual": bell_draw(splits[4], (SEQ, D), 1.0, 6.0, ((0, 32),)),
        "out_weight": bell_draw(splits[5], (QH * HEAD, D), (QH * HEAD) ** -0.5, 0.125, ((0, 4),)),
        "norm_gain": jnp.clip(1.0 + 0.18 * jax.random.normal(splits[6], (D,), jnp.float32), 0.1, 1.9),
        "expert_ids": draw_expert_ids(jax.random.fold_in(splits[12], 71), 0),
        "route_weight": jnp.clip(jnp.exp(math.log(1.0) - 1.609438 * jax.random.uniform(splits[8], (SEQ, 2), jnp.float32) ** block_levels(splits[8], (SEQ, 2), ((0, 8),), -0.2, 0.2)), 0.2, 1.0),
        "gate_proj": bell_draw(splits[9], (EXPERTS, D, FFE), D ** -0.5, 0.125, ((0, 8), (2, 4))),
        "up_proj": bell_draw(splits[10], (EXPERTS, D, FFE), D ** -0.5, 0.125, ((0, 8), (2, 4))),
        "down_proj": bell_draw(splits[11], (EXPERTS, FFE, D), FFE ** -0.5, 0.09375, ((0, 8), (1, 4))),
    }


norm_epsilon = 1e-06

def rotary(values_in, positions, head_count):
    halfway = HEAD // 2
    frequency = 10000.0 ** (-jnp.arange(halfway, dtype=jnp.float32) * 2.0 / HEAD)
    angles = positions.astype(jnp.float32)[:, None] * frequency[None, :]
    cosine = jnp.cos(angles)[:, None, :]
    sine_part = jnp.sin(angles)[:, None, :]
    reshaped = values_in.astype(jnp.float32).reshape(values_in.shape[0], head_count, HEAD)
    front_part = reshaped[..., :halfway]
    back_part = reshaped[..., halfway:]
    turned = jnp.concatenate([front_part * cosine - back_part * sine_part, back_part * cosine + front_part * sine_part], -1)
    return turned.astype(jnp.bfloat16)

def attend(query_blocks, key_pairs, value_pairs, sink_grid, key_start):
    block_count = query_blocks.shape[0]
    window_len = query_blocks.shape[1]
    scores = jnp.einsum('bqkgd,bskd->bkgqs', query_blocks.astype(jnp.float32), key_pairs.astype(jnp.float32)) * HEAD ** (-0.5)
    row_idx = jnp.arange(window_len)[:, None]
    col_idx = jnp.arange(2 * window_len)[None, :]
    distance = row_idx - col_idx + window_len
    key_pos = key_start + jnp.arange(block_count)[:, None, None] * window_len + col_idx[None]
    allowed = (distance >= 0)[None] & (distance < window_len)[None] & (key_pos >= 0)
    scores = jnp.where(allowed[:, None, None], scores, -jnp.inf)
    sink_full = sink_grid.astype(jnp.float32)[None, :, :, None]
    highest = jnp.maximum(lax.optimization_barrier(jnp.max(scores, -1)), sink_full)
    exp_scores = jnp.exp(scores - highest[..., None])
    denominator = lax.optimization_barrier(jnp.sum(exp_scores, -1)) + jnp.exp(sink_full - highest)
    probs = lax.optimization_barrier(exp_scores.astype(jnp.bfloat16)).astype(jnp.float32)
    weighted = jnp.einsum('bkgqs,bskd->bkgqd', probs, value_pairs.astype(jnp.float32))
    normalized = weighted / denominator[..., None]
    return jnp.transpose(normalized, (0, 3, 1, 2, 4)).astype(jnp.bfloat16).reshape(block_count * window_len, -1)

def reference(queries, key_rows, values, sink_logits, residual, out_weight, norm_gain, expert_ids, route_weight, gate_proj, up_proj, down_proj):
    seq_len = queries.shape[0]
    positions = jnp.arange(seq_len, dtype=jnp.int32)
    rot_query = rotary(queries, positions, QH)
    rot_key = rotary(key_rows, positions, KVH)
    group_size = QH // KVH
    block_count = seq_len // WINDOW
    padding = jnp.zeros((WINDOW, KVH, HEAD), jnp.bfloat16)
    key_blocks = jnp.concatenate([padding, rot_key], 0).reshape(block_count + 1, WINDOW, KVH, HEAD)
    value_blocks = jnp.concatenate([padding, values.reshape(seq_len, KVH, HEAD)], 0).reshape(block_count + 1, WINDOW, KVH, HEAD)
    key_pairs = jnp.concatenate([key_blocks[:-1], key_blocks[1:]], 1)
    value_pairs = jnp.concatenate([value_blocks[:-1], value_blocks[1:]], 1)
    query_blocks = rot_query.reshape(block_count, WINDOW, KVH, group_size, HEAD)
    sink_grid = sink_logits.reshape(KVH, group_size)

    def one_head(entry_item):
        query_part, key_part, value_part, sink_part = entry_item
        return attend(query_part[:, :, None], key_part[:, :, None], value_part[:, :, None], sink_part[None], -WINDOW)
    per_head = lax.map(one_head, (jnp.moveaxis(query_blocks, 2, 0), jnp.moveaxis(key_pairs, 2, 0), jnp.moveaxis(value_pairs, 2, 0), sink_grid))
    attended = jnp.moveaxis(per_head, 0, 1).reshape(seq_len, QH * HEAD)
    middle = (residual.astype(jnp.float32) + jnp.dot(attended, out_weight, preferred_element_type=jnp.float32)).astype(jnp.bfloat16)
    middle_f = middle.astype(jnp.float32)
    normed = (middle_f * lax.rsqrt(lax.optimization_barrier(jnp.mean(middle_f * middle_f, -1, keepdims=True)) + norm_epsilon) * norm_gain).astype(jnp.bfloat16)
    flattened = expert_ids.reshape(-1).astype(jnp.int32)
    most_rows = N_SP * N_TP * CAP
    slice_width = FFE // N_TP

    def one_expert(expert_index):
        matches = flattened == expert_index
        located = jnp.nonzero(matches, size=most_rows, fill_value=0)[0].astype(jnp.int32)
        is_live = jnp.arange(most_rows) < jnp.sum(matches.astype(jnp.int32))
        rows_in = normed[located // 2]
        gate_val = jnp.dot(rows_in, gate_proj[expert_index], preferred_element_type=jnp.float32)
        up_val = jnp.dot(rows_in, up_proj[expert_index], preferred_element_type=jnp.float32)
        hidden = lax.optimization_barrier((jax.nn.silu(gate_val) * up_val).astype(jnp.bfloat16)).astype(jnp.float32)
        down_slices = down_proj[expert_index].astype(jnp.float32).reshape(N_TP, slice_width, -1)
        slice_out = jnp.einsum('rsf,sfd->srd', hidden.reshape(most_rows, N_TP, slice_width), down_slices)
        slice_out = lax.optimization_barrier(slice_out.astype(jnp.bfloat16)).astype(jnp.float32)
        summed = lax.optimization_barrier(jnp.sum(slice_out, 0))
        return (located, summed * is_live[:, None].astype(jnp.float32))
    all_located, all_outputs = lax.map(one_expert, jnp.arange(N_SP, dtype=jnp.int32))
    assigned = jnp.zeros((seq_len * 2, normed.shape[1]), jnp.float32).at[all_located.reshape(-1)].add(all_outputs.reshape(-1, normed.shape[1]))
    routed = lax.optimization_barrier(jnp.sum(assigned.reshape(seq_len, 2, -1) * route_weight[..., None], 1))
    return (middle_f + routed).astype(jnp.bfloat16)
```

```python
import jax
import jax.numpy as jnp
from jax import lax
from jax.experimental import pallas as pl
from jax.experimental.pallas import tpu as pltpu
from jax.sharding import PartitionSpec as P

HEAD = 64
WINDOW = 128


norm_epsilon = 1e-06


def from_behind(block, axis, distance):
    devices = range(lax.axis_size(axis))
    route = [(i - distance, i) for i in devices if i - distance in devices]
    return lax.ppermute(block, axis, route)


def rotary(values_in, positions, head_count):
    halfway = HEAD // 2
    frequency = 10000.0 ** (-jnp.arange(halfway, dtype=jnp.float32) * 2.0 / HEAD)
    angles = positions.astype(jnp.float32)[:, None] * frequency[None, :]
    cosine = jnp.cos(angles)[:, None, :]
    sine_part = jnp.sin(angles)[:, None, :]
    reshaped = values_in.astype(jnp.float32).reshape(values_in.shape[0], head_count, HEAD)
    front_part = reshaped[..., :halfway]
    back_part = reshaped[..., halfway:]
    turned = jnp.concatenate(
        [front_part * cosine - back_part * sine_part, back_part * cosine + front_part * sine_part],
        -1,
    )
    return turned.astype(jnp.bfloat16)


def attend(query_blocks, key_pairs, value_pairs, sink_grid, key_start):
    block_count = query_blocks.shape[0]
    window_len = query_blocks.shape[1]
    scores = jnp.einsum(
        "bqkgd,bskd->bkgqs", query_blocks, key_pairs, preferred_element_type=jnp.float32
    ) * HEAD ** (-0.5)
    row_idx = jnp.arange(window_len)[:, None]
    col_idx = jnp.arange(2 * window_len)[None, :]
    distance = row_idx - col_idx + window_len
    key_pos = key_start + jnp.arange(block_count)[:, None, None] * window_len + col_idx[None]
    allowed = (distance >= 0)[None] & (distance < window_len)[None] & (key_pos >= 0)
    scores = jnp.where(allowed[:, None, None], scores, -jnp.inf)
    sink_full = sink_grid[None, :, :, None]
    highest = jnp.maximum(jnp.max(scores, -1), sink_full)
    exp_scores = jnp.exp(scores - highest[..., None])
    denominator = jnp.sum(exp_scores, -1) + jnp.exp(sink_full - highest)
    weighted = jnp.einsum(
        "bkgqs,bskd->bkgqd",
        exp_scores.astype(jnp.bfloat16),
        value_pairs,
        preferred_element_type=jnp.float32,
    )
    normalized = weighted / denominator[..., None]
    return (
        jnp.transpose(normalized, (0, 3, 1, 2, 4))
        .astype(jnp.bfloat16)
        .reshape(block_count * window_len, -1)
    )


def slot_select(picks_in, expert_count, capacity):
    flattened = picks_in.reshape(-1)
    onehot = (flattened[:, None] == jnp.arange(expert_count, dtype=jnp.int32)[None, :]).astype(
        jnp.int32
    )
    rank_of = jnp.sum(jnp.cumsum(onehot, 0) * onehot, 1) - 1
    slot_of = flattened * capacity + rank_of
    chosen = jnp.arange(expert_count * capacity, dtype=jnp.int32)[:, None] == slot_of[None, :]
    return chosen.astype(jnp.bfloat16)


def expert_part(rows_in, gate_proj, up_proj, down_proj):
    in_shape = rows_in.shape
    flattened = rows_in.reshape(-1, in_shape[-1])
    gate_val = jnp.dot(flattened, gate_proj[0], preferred_element_type=jnp.float32)
    up_val = jnp.dot(flattened, up_proj[0], preferred_element_type=jnp.float32)
    hidden = (jax.nn.silu(gate_val) * up_val).astype(jnp.bfloat16)
    return (
        jnp.dot(hidden, down_proj[0], preferred_element_type=jnp.float32)
        .astype(jnp.bfloat16)
        .reshape(in_shape)
    )


GROUPS = 4
TILE = 512
MESH = pl.DeviceIdType.MESH
VIA, ON, DIAG = 0, 1, 2


def pieces(i):
    return 2 if i == GROUPS - 1 else 1


def group_kernel(
    proj, resid, gain, extra, sel, sel_back, wg_hbm, wu_hbm, wd_hbm, out,
    wg, wu, wd, w_sem,
    rs_in, rs_s, rs_r,
    mid, normed, outb, rows,
    di_s, di_r, ag_s, ag_r, pt_s, pt_r,
    hid, outp, pr, pr_s, pr_r,
    comb, rs2, r2_s, r2_r,
    ret, back, bk_s, bk_r,
):
    sp = lax.axis_index("sp")
    t = lax.axis_index("tp")
    core = lax.rem(sp, 2)
    z = sp // 2
    tp_n, row_n, width = proj.shape
    cap = outb.shape[1]
    half = GROUPS * cap
    flip1 = t + 1 - 2 * lax.rem(t, 2)
    flip2 = lax.rem(t + 2, 4)
    flip3 = lax.rem(flip1 + 2, 4)
    peer = [t, flip1, flip2, flip3]
    via_t = flip1 + core * (flip2 - flip1)
    on_t = flip2 + core * (flip1 - flip2)
    near = [via_t, on_t, flip3]
    partner = sp + 1 - 2 * core
    plane = [z, z + 1 - 2 * lax.rem(z, 2), lax.rem(z + 2, GROUPS), GROUPS - 1 - z]

    loads = [
        pltpu.make_async_copy(a, b, w_sem.at[i])
        for i, (a, b) in enumerate(((wg_hbm, wg), (wu_hbm, wu), (wd_hbm, wd)))
    ]
    for c in loads:
        c.start()

    barrier = pltpu.get_barrier_semaphore()
    friends = [(sp, peer[d]) for d in (1, 2, 3)]
    friends += [(plane[i] * 2 + core, t) for i in (1, 2, 3)] + [(partner, t)]
    for dev in friends:
        pl.semaphore_signal(barrier, inc=1, device_id=dev, device_id_type=MESH)
    pl.semaphore_wait(barrier, len(friends))

    sent = []

    def describe(src, dst, ss, rs, dev):
        return pltpu.make_async_remote_copy(
            src_ref=src, dst_ref=dst, send_sem=ss, recv_sem=rs, device_id=dev, device_id_type=MESH
        )

    def send(src, dst, ss, rs, dev):
        c = describe(src, dst, ss, rs, dev)
        c.start()
        sent.append(c)
        return c

    firsts = [
        send(proj.at[peer[d]], rs_in.at[d - 1], rs_s.at[d - 1], rs_r.at[d - 1], (sp, peer[d]))
        for d in (3, 1, 2)
    ]
    for c in firsts:
        c.wait_recv()
    total = resid[...].astype(jnp.float32) + (
        proj[t].astype(jnp.float32)
        + rs_in[0].astype(jnp.float32)
        + rs_in[1].astype(jnp.float32)
        + rs_in[2].astype(jnp.float32)
    )
    middle = total.astype(jnp.bfloat16)
    mid[...] = middle
    mf = middle.astype(jnp.float32)
    scale = lax.rsqrt(jnp.mean(mf * mf, -1, keepdims=True) + norm_epsilon)
    normed[:, :width] = (mf * scale * gain[...]).astype(jnp.bfloat16)
    normed[:, width:] = extra[...]

    def block(tt, cc, zz):
        return rows.at[zz, pl.ds(pl.multiple_of((cc * tp_n + tt) * cap, cap), cap)]

    def pack(g):
        s = sel[pl.ds(pl.multiple_of(g * cap, cap), cap), :]
        return jnp.dot(s, normed[...], preferred_element_type=jnp.float32).astype(jnp.bfloat16)

    ag = {}
    pt = {}
    swap = {}
    r2 = {}
    disp = {}
    bk = []

    def push(d, i, tt, to):
        ref = block(tt, core, plane[i])
        ag[(d, i)] = send(ref, ref, ag_s.at[d, i], ag_r.at[d, i], (sp, to))

    def across(d, i, tt):
        ref = block(tt, core, plane[i])
        pt[(d, i)] = send(ref, ref, pt_s.at[d, i], pt_r.at[d, i], (partner, t))

    def dispatch(i):
        g = plane[i]
        outb[i] = pack(g)
        disp[i] = send(outb.at[i], block(t, core, z), di_s.at[i], di_r.at[i], (2 * g + core, t))

    def spread(i):
        if i:
            disp[i].wait_recv()
        push(VIA, i, t, via_t)
        push(ON, i, t, on_t)
        across(3, i, t)

    def relay(i):
        ag[(VIA, i)].wait_recv()
        push(DIAG, i, via_t, on_t)
        across(VIA, i, via_t)

    def other(i):
        ag[(ON, i)].wait_recv()
        across(ON, i, on_t)

    def corner(i):
        ag[(DIAG, i)].wait_recv()
        across(DIAG, i, flip3)

    def widen(i):
        for d in range(4):
            pt[(d, i)].wait_recv()

        @pl.loop(0, wg.shape[1] // TILE)
        def _(n):
            cols = pl.ds(pl.multiple_of(n * TILE, TILE), TILE)
            x = rows[plane[i], :, :width]
            g = jnp.dot(x, wg[:, cols], preferred_element_type=jnp.float32)
            u = jnp.dot(x, wu[:, cols], preferred_element_type=jnp.float32)
            hid[:, cols] = (g / (1.0 + jnp.exp(-g)) * u).astype(jnp.bfloat16)

    def part_cols(i, h):
        size = width // pieces(i)
        return pl.ds(h * size, size)

    def narrow(i, h=0):
        ext = rows[plane[i], :, width:].astype(jnp.float32)
        lane = lax.broadcasted_iota(jnp.int32, ext.shape, 1)
        mine = (lane == core) | (lane == core + 2)
        weight = jnp.sum(jnp.where(mine, ext, 0.0), -1, keepdims=True)
        tiles = width // TILE // pieces(i)

        @pl.loop(h * tiles, (h + 1) * tiles)
        def _(n):
            cols = pl.ds(pl.multiple_of(n * TILE, TILE), TILE)
            y = jnp.dot(hid[...], wd[:, cols], preferred_element_type=jnp.float32)
            outp[i, :, cols] = (y * weight).astype(jnp.bfloat16)

        here = part_cols(i, h)
        other_half = outp.at[i, pl.ds(pl.multiple_of((1 - core) * half, half), half), here]
        swap[(i, h)] = send(
            other_half, pr.at[i, :, here], pr_s.at[i, h], pr_r.at[i, h], (partner, t)
        )

    def own(i, h, tt):
        here = part_cols(i, h)
        mine = pl.ds(pl.multiple_of((core * tp_n + tt) * cap, cap), cap)
        theirs = pl.ds(pl.multiple_of(tt * cap, cap), cap)
        return outp[i, mine, here].astype(jnp.float32) + pr[i, theirs, here].astype(jnp.float32)

    def ship(d, i, h, to):
        here = part_cols(i, h)
        r2[(d, i, h)] = send(
            comb.at[i, d, :, here], rs2.at[i, d, :, here],
            r2_s.at[d, i, h], r2_r.at[d, i, h], (sp, to),
        )

    def combine(i, h=0):
        here = part_cols(i, h)
        swap[(i, h)].wait_recv()
        comb[i, DIAG, :, here] = own(i, h, flip3).astype(jnp.bfloat16)
        ship(DIAG, i, h, via_t)
        comb[i, VIA, :, here] = own(i, h, via_t).astype(jnp.bfloat16)
        ship(VIA, i, h, via_t)

    def combine_on(i, h=0):
        here = part_cols(i, h)
        r2[(DIAG, i, h)].wait_recv()
        comb[i, ON, :, here] = (
            own(i, h, on_t) + rs2[i, DIAG, :, here].astype(jnp.float32)
        ).astype(jnp.bfloat16)
        ship(ON, i, h, on_t)

    def finish(i, h=0):
        here = part_cols(i, h)
        acc = own(i, h, t)
        for d in (VIA, ON):
            r2[(d, i, h)].wait_recv()
            acc = acc + rs2[i, d, :, here].astype(jnp.float32)
        if i:
            ret[i, :, here] = acc.astype(jnp.bfloat16)
            bk.append(
                send(
                    ret.at[i, :, here], back.at[z, :, here], bk_s.at[i, h], bk_r.at[i, h],
                    (2 * plane[i] + core, t),
                )
            )
        else:
            back[z] = acc.astype(jnp.bfloat16)

    block(t, core, z)[...] = pack(z)
    spread(0)
    dispatch(1)
    dispatch(2)
    dispatch(3)
    relay(0)
    spread(1)
    other(0)
    relay(1)
    corner(0)
    spread(2)
    for c in loads:
        c.wait()
    widen(0)
    other(1)
    narrow(0)
    relay(2)
    spread(3)
    corner(1)
    widen(1)
    other(2)
    narrow(1)
    relay(3)
    corner(2)
    combine(1)
    widen(2)
    combine_on(1)
    other(3)
    narrow(2)
    corner(3)
    combine(2)
    finish(1)
    widen(3)
    combine_on(2)
    narrow(3, 0)
    finish(2)
    combine(3, 0)
    narrow(3, 1)
    combine_on(3, 0)
    combine(3, 1)
    combine(0)
    finish(3, 0)
    combine_on(3, 1)
    combine_on(0)
    finish(3, 1)
    finish(0)
    for c in bk:
        c.wait_recv()
    routed = jnp.dot(
        sel_back[...], back[...].reshape(half, width), preferred_element_type=jnp.float32
    )
    out[...] = (mid[...].astype(jnp.float32) + routed).astype(jnp.bfloat16)
    for c in sent:
        c.wait_send()


def group_experts(projected, residual, norm_gain, own_ids, own_weights, gate, up, down):
    row_n, width = residual.shape
    tp_n = lax.axis_size("tp")
    expert_n = lax.axis_size("sp")
    cap = 2 * max(1, 2 * row_n // expert_n)
    group = own_ids[:, 0] // 2
    onehot = (group[:, None] == jnp.arange(GROUPS, dtype=jnp.int32)[None, :]).astype(jnp.int32)
    rank_of = jnp.sum(jnp.cumsum(onehot, 0) * onehot, 1) - 1
    slot = group * cap + rank_of
    hit = jnp.arange(GROUPS * cap, dtype=jnp.int32)[:, None] == slot[None, :]
    sel = hit.astype(jnp.bfloat16)
    odd = lax.rem(own_ids, 2)
    pair = jnp.stack(
        [jnp.sum(jnp.where(odd == p, own_weights, 0.0), 1) for p in (0, 1)], 1
    )
    high = pair.astype(jnp.bfloat16)
    low = (pair - high.astype(jnp.float32)).astype(jnp.bfloat16)
    extra = jnp.pad(jnp.concatenate([high, low], 1), ((0, 0), (0, 124)))
    ext_width = width + 128
    ff = gate.shape[-1]
    half = GROUPS * cap
    bf = jnp.bfloat16
    dma = pltpu.SemaphoreType.DMA
    vmem = pl.BlockSpec(memory_space=pltpu.VMEM)
    hbm = pl.BlockSpec(memory_space=pl.ANY)
    return pl.pallas_call(
        group_kernel,
        out_shape=jax.ShapeDtypeStruct((row_n, width), bf),
        in_specs=[vmem] * 6 + [hbm] * 3,
        out_specs=vmem,
        scratch_shapes=[
            pltpu.VMEM((width, ff), bf),
            pltpu.VMEM((width, ff), bf),
            pltpu.VMEM((ff, width), bf),
            dma((3,)),
            pltpu.VMEM((3, row_n, width), bf),
            dma((3,)),
            dma((3,)),
            pltpu.VMEM((row_n, width), bf),
            pltpu.VMEM((row_n, ext_width), bf),
            pltpu.VMEM((GROUPS, cap, ext_width), bf),
            pltpu.VMEM((GROUPS, 2 * half, ext_width), bf),
            dma((GROUPS,)),
            dma((GROUPS,)),
            dma((3, GROUPS)),
            dma((3, GROUPS)),
            dma((4, GROUPS)),
            dma((4, GROUPS)),
            pltpu.VMEM((2 * half, ff), bf),
            pltpu.VMEM((GROUPS, 2 * half, width), bf),
            pltpu.VMEM((GROUPS, half, width), bf),
            dma((GROUPS, 2)),
            dma((GROUPS, 2)),
            pltpu.VMEM((GROUPS, 3, cap, width), bf),
            pltpu.VMEM((GROUPS, 3, cap, width), bf),
            dma((3, GROUPS, 2)),
            dma((3, GROUPS, 2)),
            pltpu.VMEM((GROUPS, cap, width), bf),
            pltpu.VMEM((GROUPS, cap, width), bf),
            dma((GROUPS, 2)),
            dma((GROUPS, 2)),
        ],
        compiler_params=pltpu.CompilerParams(
            collective_id=0, has_side_effects=True, vmem_limit_bytes=56 * 2**20
        ),
    )(
        projected.reshape(tp_n, row_n, width), residual, norm_gain[None], extra, sel,
        sel.T, gate[0], up[0], down[0],
    )


def per_device(
    queries,
    key_rows,
    values,
    sink_logits,
    residual,
    out_weight,
    norm_gain,
    expert_ids,
    route_weight,
    gate_proj,
    up_proj,
    down_proj,
):
    local_len = queries.shape[0]
    q_heads = sink_logits.shape[0]
    kv_heads = key_rows.shape[1] // HEAD
    group_size = q_heads // kv_heads
    window_len = WINDOW
    seq_start = lax.axis_index("sp") * local_len
    rim_pair = jnp.stack([key_rows[local_len - window_len :], values[local_len - window_len :]])
    rim_pair = from_behind(rim_pair, "sp", 1)
    key_ext = jnp.concatenate([rim_pair[0], key_rows], 0)
    val_ext = jnp.concatenate([rim_pair[1], values], 0)
    positions = seq_start + jnp.arange(local_len, dtype=jnp.int32)
    ext_positions = seq_start - window_len + jnp.arange(local_len + window_len, dtype=jnp.int32)
    rot_query = rotary(queries, positions, q_heads)
    rot_key = rotary(key_ext, ext_positions, kv_heads)
    block_count = local_len // window_len
    query_blocks = rot_query.reshape(block_count, window_len, kv_heads, group_size, HEAD)
    key_blocks = rot_key.reshape(block_count + 1, window_len, kv_heads, HEAD)
    value_blocks = val_ext.reshape(block_count + 1, window_len, kv_heads, HEAD)
    key_pairs = jnp.concatenate([key_blocks[:-1], key_blocks[1:]], 1)
    value_pairs = jnp.concatenate([value_blocks[:-1], value_blocks[1:]], 1)
    sink_grid = sink_logits.reshape(kv_heads, group_size)
    attended = attend(query_blocks, key_pairs, value_pairs, sink_grid, seq_start - window_len)
    tok_rows = residual.shape[0]
    tp_count = lax.axis_size("tp")
    tp_index = lax.axis_index("tp")
    if tp_count == 4 and lax.axis_size("sp") == 2 * GROUPS:
        return group_experts(
            jnp.dot(attended, out_weight, preferred_element_type=jnp.float32).astype(
                jnp.bfloat16
            ),
            residual,
            norm_gain,
            lax.dynamic_slice_in_dim(expert_ids, tp_index * tok_rows, tok_rows, 0),
            lax.dynamic_slice_in_dim(route_weight, tp_index * tok_rows, tok_rows, 0),
            gate_proj,
            up_proj,
            down_proj,
        )
    projected = lax.psum_scatter(
        jnp.dot(attended, out_weight, preferred_element_type=jnp.float32).astype(jnp.bfloat16),
        "tp",
        scatter_dimension=0,
        tiled=True,
    ).astype(jnp.float32)
    middle = (residual.astype(jnp.float32) + projected).astype(jnp.bfloat16)
    middle_f = middle.astype(jnp.float32)
    normed = (
        middle_f
        * lax.rsqrt(jnp.mean(middle_f * middle_f, -1, keepdims=True) + norm_epsilon)
        * norm_gain
    ).astype(jnp.bfloat16)
    expert_count = lax.axis_size("sp")
    capacity = 2 * max(1, 2 * tok_rows // expert_count)
    model_width = normed.shape[1]
    own_ids = lax.dynamic_slice_in_dim(expert_ids, tp_index * tok_rows, tok_rows, 0)
    own_weights = lax.dynamic_slice_in_dim(route_weight, tp_index * tok_rows, tok_rows, 0)
    select = slot_select(own_ids, expert_count, capacity)
    token_select = jnp.sum(select.reshape(expert_count * capacity, tok_rows, 2), -1)
    outbound = jnp.dot(token_select, normed, preferred_element_type=jnp.float32).astype(
        jnp.bfloat16
    )
    outbound = outbound.reshape(expert_count, capacity, model_width)
    arrived = lax.all_to_all(outbound, "sp", split_axis=0, concat_axis=0, tiled=True)
    partial_out = expert_part(
        lax.all_gather(arrived, "tp", axis=0, tiled=True), gate_proj, up_proj, down_proj
    )
    partial_out = partial_out.reshape(tp_count, expert_count * capacity, model_width)
    width_parts = lax.all_to_all(partial_out, "tp", split_axis=0, concat_axis=0, tiled=True)
    summed = jnp.sum(width_parts.astype(jnp.float32), 0).reshape(
        expert_count, capacity, model_width
    )
    returned = (
        lax.all_to_all(summed.astype(jnp.bfloat16), "sp", split_axis=0, concat_axis=0, tiled=True)
        .astype(summed.dtype)
        .reshape(expert_count * capacity, model_width)
    )
    picked = jnp.dot(
        select.astype(jnp.float32).T,
        returned,
        precision=lax.Precision.HIGHEST,
        preferred_element_type=jnp.float32,
    )
    routed = jnp.sum(picked.reshape(tok_rows, 2, model_width) * own_weights[..., None], 1)
    return (middle_f + routed).astype(jnp.bfloat16)


def solution(mesh):
    return jax.shard_map(
        per_device,
        mesh=mesh,
        in_specs=(
            P("sp", "tp"),
            P("sp", "tp"),
            P("sp", "tp"),
            P("tp"),
            P(("sp", "tp"), None),
            P("tp", None),
            P(),
            P("sp", None),
            P("sp", None),
            P("sp", None, "tp"),
            P("sp", None, "tp"),
            P("sp", "tp", None),
        ),
        out_specs=P(("sp", "tp"), None),
        check_vma=False,
    )
```

```python
import jax
import jax.numpy as jnp
import numpy as np
from jax import lax
from jax.experimental import pallas as pl
from jax.experimental.pallas import tpu as pltpu
from jax.sharding import PartitionSpec as P

HEAD = 64
WINDOW = 128


norm_epsilon = 1e-06


def from_behind(block, axis, distance):
    devices = range(lax.axis_size(axis))
    route = [(i - distance, i) for i in devices if i - distance in devices]
    return lax.ppermute(block, axis, route)


def rotary(values_in, positions, head_count):
    halfway = HEAD // 2
    frequency = 10000.0 ** (-jnp.arange(halfway, dtype=jnp.float32) * 2.0 / HEAD)
    angles = positions.astype(jnp.float32)[:, None] * frequency[None, :]
    cosine = jnp.cos(angles)[:, None, :]
    sine_part = jnp.sin(angles)[:, None, :]
    reshaped = values_in.astype(jnp.float32).reshape(values_in.shape[0], head_count, HEAD)
    front_part = reshaped[..., :halfway]
    back_part = reshaped[..., halfway:]
    turned = jnp.concatenate(
        [front_part * cosine - back_part * sine_part, back_part * cosine + front_part * sine_part],
        -1,
    )
    return turned.astype(jnp.bfloat16)


def attend(query_blocks, key_pairs, value_pairs, sink_grid, key_start):
    block_count = query_blocks.shape[0]
    window_len = query_blocks.shape[1]
    scores = jnp.einsum(
        "bqkgd,bskd->bkgqs", query_blocks, key_pairs, preferred_element_type=jnp.float32
    ) * HEAD ** (-0.5)
    row_idx = jnp.arange(window_len)[:, None]
    col_idx = jnp.arange(2 * window_len)[None, :]
    distance = row_idx - col_idx + window_len
    key_pos = key_start + jnp.arange(block_count)[:, None, None] * window_len + col_idx[None]
    allowed = (distance >= 0)[None] & (distance < window_len)[None] & (key_pos >= 0)
    scores = jnp.where(allowed[:, None, None], scores, -jnp.inf)
    sink_full = sink_grid[None, :, :, None]
    highest = jnp.maximum(jnp.max(scores, -1), sink_full)
    exp_scores = jnp.exp(scores - highest[..., None])
    denominator = jnp.sum(exp_scores, -1) + jnp.exp(sink_full - highest)
    weighted = jnp.einsum(
        "bkgqs,bskd->bkgqd",
        exp_scores.astype(jnp.bfloat16),
        value_pairs,
        preferred_element_type=jnp.float32,
    )
    normalized = weighted / denominator[..., None]
    return (
        jnp.transpose(normalized, (0, 3, 1, 2, 4))
        .astype(jnp.bfloat16)
        .reshape(block_count * window_len, -1)
    )


def slot_select(picks_in, expert_count, capacity):
    flattened = picks_in.reshape(-1)
    onehot = (flattened[:, None] == jnp.arange(expert_count, dtype=jnp.int32)[None, :]).astype(
        jnp.int32
    )
    rank_of = jnp.sum(jnp.cumsum(onehot, 0) * onehot, 1) - 1
    slot_of = flattened * capacity + rank_of
    chosen = jnp.arange(expert_count * capacity, dtype=jnp.int32)[:, None] == slot_of[None, :]
    return chosen.astype(jnp.bfloat16)


def expert_part(rows_in, gate_proj, up_proj, down_proj):
    in_shape = rows_in.shape
    flattened = rows_in.reshape(-1, in_shape[-1])
    gate_val = jnp.dot(flattened, gate_proj[0], preferred_element_type=jnp.float32)
    up_val = jnp.dot(flattened, up_proj[0], preferred_element_type=jnp.float32)
    hidden = (jax.nn.silu(gate_val) * up_val).astype(jnp.bfloat16)
    return (
        jnp.dot(hidden, down_proj[0], preferred_element_type=jnp.float32)
        .astype(jnp.bfloat16)
        .reshape(in_shape)
    )


GROUPS = 4
TILE = 512
LANES = 128
MESH = pl.DeviceIdType.MESH
VIA, ON, DIAG = 0, 1, 2


PIECES = 2


def group_kernel(
    sink, q_in, k_in, v_in, turn_row, turn_base, resid, gain, ids, weights,
    wo_hbm, wg_hbm, wu_hbm, wd_hbm, out,
    wo, wg, wu, wd, w_sem,
    rim, rim_s, rim_r, asks, keys, vals, att,
    proj, rs_in, rs_s, rs_r,
    sel, ext,
    mid, normed, outb, rows,
    di_s, di_r, ag_s, ag_r, pt_s, pt_r,
    hid, outp, pr, pr_s, pr_r,
    comb, rs2, r2_s, r2_r,
    ret, back, bk_s, bk_r,
):
    sp = lax.axis_index("sp")
    t = lax.axis_index("tp")
    sp_n = lax.axis_size("sp")
    core = lax.rem(sp, 2)
    z = sp // 2
    tp_n, row_n, width = proj.shape
    cap = outb.shape[1]
    half = GROUPS * cap
    flip1 = t + 1 - 2 * lax.rem(t, 2)
    flip2 = lax.rem(t + 2, 4)
    flip3 = lax.rem(flip1 + 2, 4)
    peer = [t, flip1, flip2, flip3]
    via_t = flip1 + core * (flip2 - flip1)
    on_t = flip2 + core * (flip1 - flip2)
    partner = sp + 1 - 2 * core
    plane = [z, z + 1 - 2 * lax.rem(z, 2), lax.rem(z + 2, GROUPS), GROUPS - 1 - z]

    loads = [
        pltpu.make_async_copy(a, b, w_sem.at[i])
        for i, (a, b) in enumerate(((wo_hbm, wo), (wg_hbm, wg), (wu_hbm, wu), (wd_hbm, wd)))
    ]
    for c in loads:
        c.start()

    barrier = pltpu.get_barrier_semaphore()
    rim_peer = lax.rem(sp + 2 * core - 1 + sp_n, sp_n)
    friends = [(sp, peer[d]) for d in (1, 2, 3)]
    friends += [(plane[i] * 2 + core, t) for i in (1, 2, 3)] + [(partner, t), (rim_peer, t)]
    for dev in friends:
        pl.semaphore_signal(barrier, inc=1, device_id=dev, device_id_type=MESH)

    sent = []

    def describe(src, dst, ss, rs, dev):
        return pltpu.make_async_remote_copy(
            src_ref=src, dst_ref=dst, send_sem=ss, recv_sem=rs, device_id=dev, device_id_type=MESH
        )

    def send(src, dst, ss, rs, dev):
        c = describe(src, dst, ss, rs, dev)
        c.start()
        sent.append(c)
        return c

    bf = jnp.bfloat16
    f32 = jnp.float32
    local = q_in.shape[0]
    tiles = k_in.shape[1] // LANES
    pairs = q_in.shape[1] // LANES
    edge = WINDOW
    pad = keys.shape[1] - local - edge
    span = pad + edge + row_n

    at_sp = lax.broadcasted_iota(jnp.int32, turn_base.shape, 0) == sp
    start = jnp.sum(jnp.where(at_sp, turn_base[...], 0.0), 0, keepdims=True)
    cb, sb = start[:, :LANES], start[:, LANES:]
    cr = turn_row[:, :LANES]
    sr = turn_row[:, LANES:]
    cosine = cb * cr - sb * sr
    sine = sb * cr + cb * sr
    spot = lax.broadcasted_iota(jnp.int32, (LANES, LANES), 0)
    lane_i = lax.broadcasted_iota(jnp.int32, (LANES, LANES), 1)
    swapped = jnp.where(lax.rem(lane_i, HEAD) < HEAD // 2, lane_i + HEAD // 2, lane_i - HEAD // 2)
    exchange = (spot == swapped).astype(bf)

    def turned(x, lo):
        n = x.shape[0]
        y = jnp.dot(x, exchange, preferred_element_type=f32)
        return x.astype(f32) * cosine[lo : lo + n] + y * sine[lo : lo + n]

    def doubled(x, ref, j, lo):
        n = x.shape[0]
        moved = pltpu.roll(x, HEAD, 1)
        first = lax.broadcasted_iota(jnp.int32, x.shape, 1) < HEAD
        ref[2 * j, lo : lo + n, :] = jnp.where(first, x, moved).astype(bf)
        ref[2 * j + 1, lo : lo + n, :] = jnp.where(first, moved, x).astype(bf)

    rim_next = lax.rem(sp + 1, sp_n)
    rims = [
        describe(
            src.at[pl.ds(local - edge, edge)], rim.at[i], rim_s.at[i], rim_r.at[i], (rim_next, t)
        )
        for i, src in enumerate((k_in, v_in))
    ]

    def rim_out():
        @pl.when(sp < sp_n - 1)
        def _():
            for c in rims:
                c.start()

    def fill(k_src, v_src, lo):
        for j in range(tiles):
            cols = slice(j * LANES, (j + 1) * LANES)
            doubled(turned(k_src[:, cols], lo), keys, j, lo + pad)
            doubled(v_src[:, cols].astype(f32), vals, j, lo + pad)

    def ask():
        lane = lax.broadcasted_iota(jnp.int32, (local, LANES), 1)
        for j in range(pairs):
            q = turned(q_in[:, j * LANES : (j + 1) * LANES], edge) * HEAD ** (-0.5)
            head = [jnp.where(lane < HEAD, q, 0.0), jnp.where(lane < HEAD, 0.0, q)]
            for i in (0, 1):
                for b in range(tp_n):
                    asks[b, j, i * row_n : (i + 1) * row_n, :] = head[i][
                        b * row_n : (b + 1) * row_n
                    ].astype(bf)
        keys[:, :pad, :] = jnp.zeros((keys.shape[0], pad, LANES), bf)
        vals[:, :pad, :] = jnp.zeros((keys.shape[0], pad, LANES), bf)

    def fill_own():
        fill(k_in, v_in, edge)

    upper = t >= tp_n // 2
    turn_order = [
        jnp.where(upper, t, flip3),
        jnp.where(upper, flip3, flip2),
        jnp.where(upper, via_t, flip1),
        jnp.where(upper, on_t, t),
    ]

    def attend_block(i):
        b = turn_order[i]
        start_at = pl.multiple_of(b * row_n, row_n)
        shape = (2 * row_n, span)
        row = lax.rem(lax.broadcasted_iota(jnp.int32, shape, 0), row_n)
        col = lax.broadcasted_iota(jnp.int32, shape, 1)
        ahead = col - row
        key_pos = sp * local + b * row_n - pad - edge + col
        allowed = (ahead > pad + edge - WINDOW) & (ahead <= pad + edge) & (key_pos >= 0)
        lane = lax.broadcasted_iota(jnp.int32, (row_n, LANES), 1)
        top = lax.broadcasted_iota(jnp.int32, (2 * row_n, 1), 0) < row_n
        window = pl.ds(start_at, span)
        all_j = range(pairs)
        scores = [
            lax.dot_general(
                asks[b, j], keys[j, window, :], (((1,), (1,)), ((), ())),
                preferred_element_type=f32,
            )
            for j in all_j
        ]
        scores = [jnp.where(allowed, s, -jnp.inf) for s in scores]
        rest = [jnp.where(top, sink[2 * j], sink[2 * j + 1]) for j in all_j]
        highest = [
            jnp.maximum(jnp.max(scores[j], -1, keepdims=True), rest[j]) for j in all_j
        ]
        probs = [jnp.exp(scores[j] - highest[j]) for j in all_j]
        mixed = [
            jnp.dot(probs[j].astype(bf), vals[j, window, :], preferred_element_type=f32)
            for j in all_j
        ]
        share = [
            1.0 / (jnp.sum(probs[j], -1, keepdims=True) + jnp.exp(rest[j] - highest[j]))
            for j in all_j
        ]
        for j in all_j:
            m = mixed[j] * share[j]
            att[:, j * LANES : (j + 1) * LANES] = jnp.where(
                lane < HEAD, m[:row_n], m[row_n:]
            ).astype(bf)
        if i == 0:
            loads[0].wait()
        proj[b] = jnp.dot(att[...], wo[...], preferred_element_type=f32).astype(bf)

    def give(i):
        b = turn_order[i]
        slot = jnp.where(b == flip3, DIAG, VIA)

        @pl.when((b != t) & (b != on_t))
        def _():
            describe(
                proj.at[b], rs_in.at[slot], rs_s.at[slot], rs_r.at[slot], (sp, via_t)
            ).start()

    def given(slot, to):
        return describe(proj.at[0], rs_in.at[slot], rs_s.at[slot], rs_r.at[slot], (sp, to))

    def give_on():
        given(DIAG, via_t).wait_recv()
        proj[on_t] = (proj[on_t].astype(f32) + rs_in[DIAG].astype(f32)).astype(bf)
        send(proj.at[on_t], rs_in.at[ON], rs_s.at[ON], rs_r.at[ON], (sp, on_t))

    def rim_in(now):
        @pl.when(now & (sp > 0))
        def _():
            for c in rims:
                c.wait_recv()

        @pl.when(now & (sp == 0))
        def _():
            rim[...] = jnp.zeros(rim.shape, bf)

        @pl.when(now)
        def _():
            fill(rim.at[0], rim.at[1], 0)

    def slots():
        def mine(x):
            x = jnp.broadcast_to(x, (8, x.shape[1]))
            x = jnp.where(t >= 2, x[:, LANES:], x[:, :LANES])
            return jnp.where(lax.rem(t, 2) == 1, pltpu.roll(x, row_n, 1), x)

        picks = [mine(ids[k : k + 1, :]) for k in (0, 1)]
        parts = [mine(weights[k : k + 1, :]) for k in (0, 1)]
        lane = lax.broadcasted_iota(jnp.int32, (8, LANES), 1)
        sub = lax.broadcasted_iota(jnp.int32, (8, LANES), 0)
        group = jnp.where(lane < row_n, picks[0] // 2, -1)
        hit = sub == group
        before = (spot < lane_i).astype(bf)
        rank = jnp.dot(hit.astype(f32).astype(bf), before, preferred_element_type=f32)
        rank = jnp.sum(jnp.where(hit, rank, 0.0), 0, keepdims=True).astype(jnp.int32)
        slot = group[0:1] * cap + rank
        slot = jnp.where(lane[0:1] < row_n, slot, -1)
        chosen = (spot == jnp.broadcast_to(slot, (LANES, LANES))).astype(f32).astype(bf)
        sel[0] = chosen
        sel[1] = lax.dot_general(
            (spot == lane_i).astype(f32).astype(bf), chosen, (((1,), (1,)), ((), ())),
            preferred_element_type=f32,
        ).astype(bf)
        table = jnp.zeros((8, LANES), f32)
        for p in (0, 1):
            w = sum(jnp.where(lax.rem(picks[k], 2) == p, parts[k], 0.0) for k in (0, 1))
            w = jnp.where(lane < row_n, w, 0.0)
            high = w.astype(bf).astype(f32)
            table = jnp.where(sub == p, high, table)
            table = jnp.where(sub == p + 2, w - high, table)
        table = jnp.concatenate([table, jnp.zeros((LANES - 8, LANES), f32)], 0).astype(bf)
        ext[...] = lax.dot_general(
            chosen, table, (((1,), (1,)), ((), ())), preferred_element_type=f32
        ).astype(bf)

    def meet():
        pl.semaphore_wait(barrier, len(friends))

    def gathered():
        given(VIA, via_t).wait_recv()
        given(ON, on_t).wait_recv()

    ask()
    slots()
    meet()
    rim_out()
    fill_own()
    attend_block(0)
    give(0)
    rim_in(upper)
    attend_block(1)
    give(1)
    rim_in(t < tp_n // 2)
    attend_block(2)
    give(2)
    attend_block(3)
    give(3)
    give_on()
    gathered()
    total = resid[...].astype(f32) + (
        proj[t].astype(f32) + rs_in[VIA].astype(f32) + rs_in[ON].astype(f32)
    )
    middle = total.astype(bf)
    mid[...] = middle
    mf = middle.astype(f32)
    scale = lax.rsqrt(jnp.mean(mf * mf, -1, keepdims=True) + norm_epsilon)
    normed[...] = (mf * scale * gain[...]).astype(bf)

    def block(tt, cc, zz):
        return rows.at[zz, pl.ds(pl.multiple_of((cc * tp_n + tt) * cap, cap), cap)]

    def pack(g, ref):
        spots = pl.ds(pl.multiple_of(g * cap, cap), cap)
        ref[:, :width] = jnp.dot(
            sel[0, spots, :row_n], normed[...], preferred_element_type=f32
        ).astype(bf)
        ref[:, width:] = ext[spots, :]

    ag = {}
    pt = {}
    swap = {}
    r2 = {}
    disp = {}
    bk = []

    def push(d, i, tt, to):
        ref = block(tt, core, plane[i])
        ag[(d, i)] = send(ref, ref, ag_s.at[d, i], ag_r.at[d, i], (sp, to))

    def across(d, i, tt):
        ref = block(tt, core, plane[i])
        pt[(d, i)] = send(ref, ref, pt_s.at[d, i], pt_r.at[d, i], (partner, t))

    def dispatch(i):
        g = plane[i]
        pack(g, outb.at[i])
        disp[i] = send(outb.at[i], block(t, core, z), di_s.at[i], di_r.at[i], (2 * g + core, t))

    def spread(i):
        if i:
            disp[i].wait_recv()
        push(VIA, i, t, via_t)
        push(ON, i, t, on_t)
        across(3, i, t)

    def relay(i):
        ag[(VIA, i)].wait_recv()
        push(DIAG, i, via_t, on_t)
        across(VIA, i, via_t)

    def other(i):
        ag[(ON, i)].wait_recv()
        across(ON, i, on_t)

    def corner(i):
        ag[(DIAG, i)].wait_recv()
        across(DIAG, i, flip3)

    def widen(i, h):
        if h == 0:
            for d in range(4):
                pt[(d, i)].wait_recv()
        if i == 0 and h == 0:
            for c in loads[1:]:
                c.wait()
        size = wg.shape[1] // PIECES
        cols = pl.ds(h * size, size)
        x = rows[plane[i], :, :width]
        g = jnp.dot(x, wg[:, cols], preferred_element_type=jnp.float32)
        u = jnp.dot(x, wu[:, cols], preferred_element_type=jnp.float32)
        hid[i, :, cols] = (g / (1.0 + jnp.exp(-g)) * u).astype(jnp.bfloat16)

    def part_cols(i, h):
        size = width // PIECES
        return pl.ds(h * size, size)

    def narrow(i, h):
        ext = rows[plane[i], :, width:].astype(jnp.float32)
        lane = lax.broadcasted_iota(jnp.int32, ext.shape, 1)
        mine = (lane == core) | (lane == core + 2)
        weight = jnp.sum(jnp.where(mine, ext, 0.0), -1, keepdims=True)
        tiles = width // TILE // PIECES

        @pl.loop(h * tiles, (h + 1) * tiles)
        def _(n):
            cols = pl.ds(pl.multiple_of(n * TILE, TILE), TILE)
            y = jnp.dot(hid[i], wd[:, cols], preferred_element_type=jnp.float32)
            outp[i, :, cols] = (y * weight).astype(jnp.bfloat16)

        here = part_cols(i, h)
        other_half = outp.at[i, pl.ds(pl.multiple_of((1 - core) * half, half), half), here]
        swap[(i, h)] = send(
            other_half, pr.at[i, :, here], pr_s.at[i, h], pr_r.at[i, h], (partner, t)
        )

    def own(i, h, tt):
        here = part_cols(i, h)
        mine = pl.ds(pl.multiple_of((core * tp_n + tt) * cap, cap), cap)
        theirs = pl.ds(pl.multiple_of(tt * cap, cap), cap)
        return outp[i, mine, here].astype(jnp.float32) + pr[i, theirs, here].astype(jnp.float32)

    def ship(d, i, h, to):
        here = part_cols(i, h)
        r2[(d, i, h)] = send(
            comb.at[i, d, :, here], rs2.at[i, d, :, here],
            r2_s.at[d, i, h], r2_r.at[d, i, h], (sp, to),
        )

    def combine(i, h):
        here = part_cols(i, h)
        swap[(i, h)].wait_recv()
        comb[i, DIAG, :, here] = own(i, h, flip3).astype(jnp.bfloat16)
        ship(DIAG, i, h, via_t)
        comb[i, VIA, :, here] = own(i, h, via_t).astype(jnp.bfloat16)
        ship(VIA, i, h, via_t)

    def combine_on(i, h):
        here = part_cols(i, h)
        r2[(DIAG, i, h)].wait_recv()
        comb[i, ON, :, here] = (
            own(i, h, on_t) + rs2[i, DIAG, :, here].astype(jnp.float32)
        ).astype(jnp.bfloat16)
        ship(ON, i, h, on_t)

    def finish(i, h):
        here = part_cols(i, h)
        acc = own(i, h, t)
        for d in (VIA, ON):
            r2[(d, i, h)].wait_recv()
            acc = acc + rs2[i, d, :, here].astype(jnp.float32)
        if i:
            ret[i, :, here] = acc.astype(jnp.bfloat16)
            bk.append(
                send(
                    ret.at[i, :, here], back.at[z, :, here], bk_s.at[i, h], bk_r.at[i, h],
                    (2 * plane[i] + core, t),
                )
            )
        else:
            back[z, :, here] = acc.astype(jnp.bfloat16)

    pack(z, block(t, core, z))
    spread(0)
    dispatch(1)
    dispatch(2)
    dispatch(3)
    relay(0)
    other(0)
    spread(1)
    spread(2)
    corner(0)
    relay(1)
    widen(0, 0)
    other(1)
    widen(0, 1)
    relay(2)
    spread(3)
    narrow(0, 0)
    corner(1)
    other(2)
    narrow(0, 1)
    widen(1, 0)
    combine(0, 0)
    widen(1, 1)
    corner(2)
    narrow(1, 0)
    relay(3)
    widen(2, 0)
    widen(2, 1)
    combine(1, 0)
    other(3)
    narrow(2, 0)
    combine(0, 1)
    corner(3)
    narrow(2, 1)
    combine(2, 0)
    widen(3, 0)
    combine_on(1, 0)
    combine(2, 1)
    widen(3, 1)
    narrow(3, 0)
    combine_on(2, 0)
    narrow(3, 1)
    combine(3, 0)
    finish(1, 0)
    narrow(1, 1)
    combine(3, 1)
    combine(1, 1)
    finish(2, 0)
    combine_on(3, 0)
    combine_on(3, 1)
    combine_on(2, 1)
    combine_on(1, 1)
    finish(3, 0)
    finish(3, 1)
    combine_on(0, 0)
    finish(2, 1)
    finish(1, 1)
    combine_on(0, 1)
    finish(0, 0)
    finish(0, 1)
    for c in bk:
        c.wait_recv()
    routed = jnp.dot(
        sel[1, :row_n, :], back[...].reshape(half, width), preferred_element_type=f32
    )
    out[...] = (mid[...].astype(jnp.float32) + routed).astype(jnp.bfloat16)
    for c in sent:
        c.wait_send()
    for slot in (VIA, DIAG):
        given(slot, via_t).wait_send()

    @pl.when(sp < sp_n - 1)
    def _():
        for c in rims:
            c.wait_send()


def group_layer(
    queries, key_rows, values, sink_logits, residual, out_weight, norm_gain, expert_ids,
    route_weight, gate, up, down,
):
    row_n, width = residual.shape
    local = queries.shape[0]
    tp_n = lax.axis_size("tp")
    expert_n = lax.axis_size("sp")
    cap = 2 * max(1, 2 * row_n // expert_n)
    ext_width = width + LANES
    ff = gate.shape[-1]
    half = GROUPS * cap
    kv_heads = key_rows.shape[1] // HEAD
    frequency = 10000.0 ** (-(np.arange(LANES) % (HEAD // 2)) * 2.0 / HEAD)
    sign = np.where(np.arange(LANES) % HEAD < HEAD // 2, -1.0, 1.0)

    def turns(positions):
        angle = positions[:, None] * frequency[None, :]
        return jnp.asarray(
            np.concatenate([np.cos(angle), np.sin(angle) * sign], 1), jnp.float32
        )

    turn_row = turns(np.arange(local + WINDOW) - float(WINDOW))
    turn_base = turns(np.arange(expert_n) * float(local))
    bf = jnp.bfloat16
    dma = pltpu.SemaphoreType.DMA
    vmem = pl.BlockSpec(memory_space=pltpu.VMEM)
    smem = pl.BlockSpec(memory_space=pltpu.SMEM)
    hbm = pl.BlockSpec(memory_space=pl.ANY)
    return pl.pallas_call(
        group_kernel,
        out_shape=jax.ShapeDtypeStruct((row_n, width), bf),
        in_specs=[smem] + [vmem] * 9 + [hbm] * 4,
        out_specs=vmem,
        scratch_shapes=[
            pltpu.VMEM(out_weight.shape, bf),
            pltpu.VMEM((width, ff), bf),
            pltpu.VMEM((width, ff), bf),
            pltpu.VMEM((ff, width), bf),
            dma((4,)),
            pltpu.VMEM((2, WINDOW, key_rows.shape[1]), bf),
            dma((2,)),
            dma((2,)),
            pltpu.VMEM((tp_n, queries.shape[1] // LANES, 2 * row_n, LANES), bf),
            pltpu.VMEM((kv_heads, local + WINDOW + row_n, LANES), bf),
            pltpu.VMEM((kv_heads, local + WINDOW + row_n, LANES), bf),
            pltpu.VMEM((row_n, queries.shape[1]), bf),
            pltpu.VMEM((tp_n, row_n, width), bf),
            pltpu.VMEM((3, row_n, width), bf),
            dma((3,)),
            dma((3,)),
            pltpu.VMEM((2, LANES, LANES), bf),
            pltpu.VMEM((LANES, LANES), bf),
            pltpu.VMEM((row_n, width), bf),
            pltpu.VMEM((row_n, width), bf),
            pltpu.VMEM((GROUPS, cap, ext_width), bf),
            pltpu.VMEM((GROUPS, 2 * half, ext_width), bf),
            dma((GROUPS,)),
            dma((GROUPS,)),
            dma((3, GROUPS)),
            dma((3, GROUPS)),
            dma((4, GROUPS)),
            dma((4, GROUPS)),
            pltpu.VMEM((GROUPS, 2 * half, ff), bf),
            pltpu.VMEM((GROUPS, 2 * half, width), bf),
            pltpu.VMEM((GROUPS, half, width), bf),
            dma((GROUPS, 2)),
            dma((GROUPS, 2)),
            pltpu.VMEM((GROUPS, 3, cap, width), bf),
            pltpu.VMEM((GROUPS, 3, cap, width), bf),
            dma((3, GROUPS, 2)),
            dma((3, GROUPS, 2)),
            pltpu.VMEM((GROUPS, cap, width), bf),
            pltpu.VMEM((GROUPS, cap, width), bf),
            dma((GROUPS, 2)),
            dma((GROUPS, 2)),
        ],
        compiler_params=pltpu.CompilerParams(
            collective_id=0, has_side_effects=True, vmem_limit_bytes=60 * 2**20
        ),
    )(
        sink_logits, queries, key_rows, values, turn_row, turn_base, residual, norm_gain[None],
        expert_ids.T, route_weight.T, out_weight, gate[0], up[0], down[0],
    )


def per_device(
    queries,
    key_rows,
    values,
    sink_logits,
    residual,
    out_weight,
    norm_gain,
    expert_ids,
    route_weight,
    gate_proj,
    up_proj,
    down_proj,
):
    local_len = queries.shape[0]
    if lax.axis_size("tp") == 4 and lax.axis_size("sp") == 2 * GROUPS:
        return group_layer(
            queries, key_rows, values, sink_logits, residual, out_weight, norm_gain,
            expert_ids, route_weight, gate_proj, up_proj, down_proj,
        )
    q_heads = sink_logits.shape[0]
    kv_heads = key_rows.shape[1] // HEAD
    group_size = q_heads // kv_heads
    window_len = WINDOW
    seq_start = lax.axis_index("sp") * local_len
    rim_pair = jnp.stack([key_rows[local_len - window_len :], values[local_len - window_len :]])
    rim_pair = from_behind(rim_pair, "sp", 1)
    key_ext = jnp.concatenate([rim_pair[0], key_rows], 0)
    val_ext = jnp.concatenate([rim_pair[1], values], 0)
    positions = seq_start + jnp.arange(local_len, dtype=jnp.int32)
    ext_positions = seq_start - window_len + jnp.arange(local_len + window_len, dtype=jnp.int32)
    rot_query = rotary(queries, positions, q_heads)
    rot_key = rotary(key_ext, ext_positions, kv_heads)
    block_count = local_len // window_len
    query_blocks = rot_query.reshape(block_count, window_len, kv_heads, group_size, HEAD)
    key_blocks = rot_key.reshape(block_count + 1, window_len, kv_heads, HEAD)
    value_blocks = val_ext.reshape(block_count + 1, window_len, kv_heads, HEAD)
    key_pairs = jnp.concatenate([key_blocks[:-1], key_blocks[1:]], 1)
    value_pairs = jnp.concatenate([value_blocks[:-1], value_blocks[1:]], 1)
    sink_grid = sink_logits.reshape(kv_heads, group_size)
    attended = attend(query_blocks, key_pairs, value_pairs, sink_grid, seq_start - window_len)
    tok_rows = residual.shape[0]
    tp_count = lax.axis_size("tp")
    tp_index = lax.axis_index("tp")
    projected = lax.psum_scatter(
        jnp.dot(attended, out_weight, preferred_element_type=jnp.float32).astype(jnp.bfloat16),
        "tp",
        scatter_dimension=0,
        tiled=True,
    ).astype(jnp.float32)
    middle = (residual.astype(jnp.float32) + projected).astype(jnp.bfloat16)
    middle_f = middle.astype(jnp.float32)
    normed = (
        middle_f
        * lax.rsqrt(jnp.mean(middle_f * middle_f, -1, keepdims=True) + norm_epsilon)
        * norm_gain
    ).astype(jnp.bfloat16)
    expert_count = lax.axis_size("sp")
    capacity = 2 * max(1, 2 * tok_rows // expert_count)
    model_width = normed.shape[1]
    own_ids = lax.dynamic_slice_in_dim(expert_ids, tp_index * tok_rows, tok_rows, 0)
    own_weights = lax.dynamic_slice_in_dim(route_weight, tp_index * tok_rows, tok_rows, 0)
    select = slot_select(own_ids, expert_count, capacity)
    token_select = jnp.sum(select.reshape(expert_count * capacity, tok_rows, 2), -1)
    outbound = jnp.dot(token_select, normed, preferred_element_type=jnp.float32).astype(
        jnp.bfloat16
    )
    outbound = outbound.reshape(expert_count, capacity, model_width)
    arrived = lax.all_to_all(outbound, "sp", split_axis=0, concat_axis=0, tiled=True)
    partial_out = expert_part(
        lax.all_gather(arrived, "tp", axis=0, tiled=True), gate_proj, up_proj, down_proj
    )
    partial_out = partial_out.reshape(tp_count, expert_count * capacity, model_width)
    width_parts = lax.all_to_all(partial_out, "tp", split_axis=0, concat_axis=0, tiled=True)
    summed = jnp.sum(width_parts.astype(jnp.float32), 0).reshape(
        expert_count, capacity, model_width
    )
    returned = (
        lax.all_to_all(summed.astype(jnp.bfloat16), "sp", split_axis=0, concat_axis=0, tiled=True)
        .astype(summed.dtype)
        .reshape(expert_count * capacity, model_width)
    )
    picked = jnp.dot(
        select.astype(jnp.float32).T,
        returned,
        precision=lax.Precision.HIGHEST,
        preferred_element_type=jnp.float32,
    )
    routed = jnp.sum(picked.reshape(tok_rows, 2, model_width) * own_weights[..., None], 1)
    return (middle_f + routed).astype(jnp.bfloat16)


def solution(mesh):
    return jax.shard_map(
        per_device,
        mesh=mesh,
        in_specs=(
            P("sp", "tp"),
            P("sp", "tp"),
            P("sp", "tp"),
            P("tp"),
            P(("sp", "tp"), None),
            P("tp", None),
            P(),
            P("sp", None),
            P("sp", None),
            P("sp", None, "tp"),
            P("sp", None, "tp"),
            P("sp", "tp", None),
        ),
        out_specs=P(("sp", "tp"), None),
        check_vma=False,
    )
```

```python
import jax
import jax.numpy as jnp
import numpy as np
from jax import lax
from jax.experimental import pallas as pl
from jax.experimental.pallas import tpu as pltpu
from jax.sharding import PartitionSpec as P

HEAD = 64
WINDOW = 128


norm_epsilon = 1e-06


def from_behind(block, axis, distance):
    devices = range(lax.axis_size(axis))
    route = [(i - distance, i) for i in devices if i - distance in devices]
    return lax.ppermute(block, axis, route)


def rotary(values_in, positions, head_count):
    halfway = HEAD // 2
    frequency = 10000.0 ** (-jnp.arange(halfway, dtype=jnp.float32) * 2.0 / HEAD)
    angles = positions.astype(jnp.float32)[:, None] * frequency[None, :]
    cosine = jnp.cos(angles)[:, None, :]
    sine_part = jnp.sin(angles)[:, None, :]
    reshaped = values_in.astype(jnp.float32).reshape(values_in.shape[0], head_count, HEAD)
    front_part = reshaped[..., :halfway]
    back_part = reshaped[..., halfway:]
    turned = jnp.concatenate(
        [front_part * cosine - back_part * sine_part, back_part * cosine + front_part * sine_part],
        -1,
    )
    return turned.astype(jnp.bfloat16)


def attend(query_blocks, key_pairs, value_pairs, sink_grid, key_start):
    block_count = query_blocks.shape[0]
    window_len = query_blocks.shape[1]
    scores = jnp.einsum(
        "bqkgd,bskd->bkgqs", query_blocks, key_pairs, preferred_element_type=jnp.float32
    ) * HEAD ** (-0.5)
    row_idx = jnp.arange(window_len)[:, None]
    col_idx = jnp.arange(2 * window_len)[None, :]
    distance = row_idx - col_idx + window_len
    key_pos = key_start + jnp.arange(block_count)[:, None, None] * window_len + col_idx[None]
    allowed = (distance >= 0)[None] & (distance < window_len)[None] & (key_pos >= 0)
    scores = jnp.where(allowed[:, None, None], scores, -jnp.inf)
    sink_full = sink_grid[None, :, :, None]
    highest = jnp.maximum(jnp.max(scores, -1), sink_full)
    exp_scores = jnp.exp(scores - highest[..., None])
    denominator = jnp.sum(exp_scores, -1) + jnp.exp(sink_full - highest)
    weighted = jnp.einsum(
        "bkgqs,bskd->bkgqd",
        exp_scores.astype(jnp.bfloat16),
        value_pairs,
        preferred_element_type=jnp.float32,
    )
    normalized = weighted / denominator[..., None]
    return (
        jnp.transpose(normalized, (0, 3, 1, 2, 4))
        .astype(jnp.bfloat16)
        .reshape(block_count * window_len, -1)
    )


def slot_select(picks_in, expert_count, capacity):
    flattened = picks_in.reshape(-1)
    onehot = (flattened[:, None] == jnp.arange(expert_count, dtype=jnp.int32)[None, :]).astype(
        jnp.int32
    )
    rank_of = jnp.sum(jnp.cumsum(onehot, 0) * onehot, 1) - 1
    slot_of = flattened * capacity + rank_of
    chosen = jnp.arange(expert_count * capacity, dtype=jnp.int32)[:, None] == slot_of[None, :]
    return chosen.astype(jnp.bfloat16)


def expert_part(rows_in, gate_proj, up_proj, down_proj):
    in_shape = rows_in.shape
    flattened = rows_in.reshape(-1, in_shape[-1])
    gate_val = jnp.dot(flattened, gate_proj[0], preferred_element_type=jnp.float32)
    up_val = jnp.dot(flattened, up_proj[0], preferred_element_type=jnp.float32)
    hidden = (jax.nn.silu(gate_val) * up_val).astype(jnp.bfloat16)
    return (
        jnp.dot(hidden, down_proj[0], preferred_element_type=jnp.float32)
        .astype(jnp.bfloat16)
        .reshape(in_shape)
    )


GROUPS = 4
TILE = 512
LANES = 128
MESH = pl.DeviceIdType.MESH
VIA, ON, DIAG = 0, 1, 2


PIECES = 2


def group_kernel(
    sink_hbm, q_hbm, k_hbm, v_hbm, row_hbm, base_hbm, resid_hbm, gain_hbm, ids_hbm, weights_hbm,
    wo_hbm, wg_hbm, wu_hbm, wd_hbm, out,
    sink, q_in, k_in, v_in, turn_row, turn_base, resid, gain, ids, weights, in_sem,
    wo, wg, wu, wd, w_sem,
    rim, rim_s, rim_r, asks, keys, vals, att,
    proj, rs_in, rs_s, rs_r,
    sel, ext,
    mid, normed, outb, rows,
    di_s, di_r, ag_s, ag_r, pt_s, pt_r,
    hid, outp, pr, pr_s, pr_r,
    comb, rs2, r2_s, r2_r,
    ret, back, bk_s, bk_r,
):
    sp = lax.axis_index("sp")
    t = lax.axis_index("tp")
    sp_n = lax.axis_size("sp")
    core = lax.rem(sp, 2)
    z = sp // 2
    tp_n, row_n, width = proj.shape
    cap = outb.shape[1]
    half = GROUPS * cap
    flip1 = t + 1 - 2 * lax.rem(t, 2)
    flip2 = lax.rem(t + 2, 4)
    flip3 = lax.rem(flip1 + 2, 4)
    peer = [t, flip1, flip2, flip3]
    via_t = flip1 + core * (flip2 - flip1)
    on_t = flip2 + core * (flip1 - flip2)
    partner = sp + 1 - 2 * core
    plane = [z, z + 1 - 2 * lax.rem(z, 2), lax.rem(z + 2, GROUPS), GROUPS - 1 - z]

    barrier = pltpu.get_barrier_semaphore()
    rim_peer = lax.rem(sp + 2 * core - 1 + sp_n, sp_n)
    friends = [(sp, peer[d]) for d in (1, 2, 3)]
    friends += [(plane[i] * 2 + core, t) for i in (1, 2, 3)] + [(partner, t), (rim_peer, t)]
    for dev in friends:
        pl.semaphore_signal(barrier, inc=1, device_id=dev, device_id_type=MESH)

    moves = (
        (row_hbm, turn_row), (base_hbm, turn_base), (q_hbm, q_in), (k_hbm, k_in), (v_hbm, v_in),
        (ids_hbm, ids), (weights_hbm, weights), (sink_hbm, sink),
        (resid_hbm, resid), (gain_hbm, gain),
    )
    feeds = [pltpu.make_async_copy(a, b, in_sem.at[i]) for i, (a, b) in enumerate(moves)]
    loads = [
        pltpu.make_async_copy(a, b, w_sem.at[i])
        for i, (a, b) in enumerate(((wo_hbm, wo), (wg_hbm, wg), (wu_hbm, wu), (wd_hbm, wd)))
    ]
    for c in feeds + loads:
        c.start()

    sent = []

    def describe(src, dst, ss, rs, dev):
        return pltpu.make_async_remote_copy(
            src_ref=src, dst_ref=dst, send_sem=ss, recv_sem=rs, device_id=dev, device_id_type=MESH
        )

    def send(src, dst, ss, rs, dev):
        c = describe(src, dst, ss, rs, dev)
        c.start()
        sent.append(c)
        return c

    bf = jnp.bfloat16
    f32 = jnp.float32
    local = q_in.shape[0]
    tiles = k_in.shape[1] // LANES
    pairs = q_in.shape[1] // LANES
    edge = WINDOW
    pad = keys.shape[1] - local - edge
    span = pad + edge + row_n

    for c in feeds[:-2]:
        c.wait()
    at_sp = lax.broadcasted_iota(jnp.int32, turn_base.shape, 0) == sp
    start = jnp.sum(jnp.where(at_sp, turn_base[...], 0.0), 0, keepdims=True)
    cb, sb = start[:, :LANES], start[:, LANES:]
    cr = turn_row[:, :LANES]
    sr = turn_row[:, LANES:]
    cosine = cb * cr - sb * sr
    sine = sb * cr + cb * sr
    spot = lax.broadcasted_iota(jnp.int32, (LANES, LANES), 0)
    lane_i = lax.broadcasted_iota(jnp.int32, (LANES, LANES), 1)
    swapped = jnp.where(lax.rem(lane_i, HEAD) < HEAD // 2, lane_i + HEAD // 2, lane_i - HEAD // 2)
    exchange = (spot == swapped).astype(bf)

    def turned(x, lo):
        n = x.shape[0]
        y = jnp.dot(x, exchange, preferred_element_type=f32)
        return x.astype(f32) * cosine[lo : lo + n] + y * sine[lo : lo + n]

    def doubled(x, ref, j, lo):
        n = x.shape[0]
        moved = pltpu.roll(x, HEAD, 1)
        first = lax.broadcasted_iota(jnp.int32, x.shape, 1) < HEAD
        ref[2 * j, lo : lo + n, :] = jnp.where(first, x, moved).astype(bf)
        ref[2 * j + 1, lo : lo + n, :] = jnp.where(first, moved, x).astype(bf)

    rim_next = lax.rem(sp + 1, sp_n)
    rims = [
        describe(
            src.at[pl.ds(local - edge, edge)], rim.at[i], rim_s.at[i], rim_r.at[i], (rim_next, t)
        )
        for i, src in enumerate((k_in, v_in))
    ]

    def rim_out():
        @pl.when(sp < sp_n - 1)
        def _():
            for c in rims:
                c.start()

    def fill(k_src, v_src, lo):
        for j in range(tiles):
            cols = slice(j * LANES, (j + 1) * LANES)
            doubled(turned(k_src[:, cols], lo), keys, j, lo + pad)
            doubled(v_src[:, cols].astype(f32), vals, j, lo + pad)

    def ask():
        lane = lax.broadcasted_iota(jnp.int32, (local, LANES), 1)
        for j in range(pairs):
            q = turned(q_in[:, j * LANES : (j + 1) * LANES], edge) * HEAD ** (-0.5)
            head = [jnp.where(lane < HEAD, q, 0.0), jnp.where(lane < HEAD, 0.0, q)]
            for i in (0, 1):
                for b in range(tp_n):
                    asks[b, j, i * row_n : (i + 1) * row_n, :] = head[i][
                        b * row_n : (b + 1) * row_n
                    ].astype(bf)
        keys[:, :pad, :] = jnp.zeros((keys.shape[0], pad, LANES), bf)
        vals[:, :pad, :] = jnp.zeros((keys.shape[0], pad, LANES), bf)

    def fill_own():
        fill(k_in, v_in, edge)

    upper = t >= tp_n // 2
    turn_order = [
        jnp.where(upper, t, flip3),
        jnp.where(upper, flip3, flip2),
        flip1,
        jnp.where(upper, flip2, t),
    ]

    def attend_block(i):
        b = turn_order[i]
        start_at = pl.multiple_of(b * row_n, row_n)
        shape = (2 * row_n, span)
        row = lax.rem(lax.broadcasted_iota(jnp.int32, shape, 0), row_n)
        col = lax.broadcasted_iota(jnp.int32, shape, 1)
        ahead = col - row
        key_pos = sp * local + b * row_n - pad - edge + col
        allowed = (ahead > pad + edge - WINDOW) & (ahead <= pad + edge) & (key_pos >= 0)
        lane = lax.broadcasted_iota(jnp.int32, (row_n, LANES), 1)
        top = lax.broadcasted_iota(jnp.int32, (2 * row_n, 1), 0) < row_n
        window = pl.ds(start_at, span)
        all_j = range(pairs)
        scores = [
            lax.dot_general(
                asks[b, j], keys[j, window, :], (((1,), (1,)), ((), ())),
                preferred_element_type=f32,
            )
            for j in all_j
        ]
        scores = [jnp.where(allowed, s, -jnp.inf) for s in scores]
        rest = [jnp.where(top, sink[2 * j], sink[2 * j + 1]) for j in all_j]
        highest = [
            jnp.maximum(jnp.max(scores[j], -1, keepdims=True), rest[j]) for j in all_j
        ]
        probs = [jnp.exp(scores[j] - highest[j]) for j in all_j]
        mixed = [
            jnp.dot(probs[j].astype(bf), vals[j, window, :], preferred_element_type=f32)
            for j in all_j
        ]
        share = [
            1.0 / (jnp.sum(probs[j], -1, keepdims=True) + jnp.exp(rest[j] - highest[j]))
            for j in all_j
        ]
        for j in all_j:
            m = mixed[j] * share[j]
            att[:, j * LANES : (j + 1) * LANES] = jnp.where(
                lane < HEAD, m[:row_n], m[row_n:]
            ).astype(bf)
        if i == 0:
            loads[0].wait()
        proj[b] = jnp.dot(att[...], wo[...], preferred_element_type=f32).astype(bf)

    lead = [via_t, on_t]

    def part(h):
        size = width // 2
        return slice(h * size, (h + 1) * size)

    def given(slot, h, b, to):
        return describe(
            proj.at[b, :, part(h)], rs_in.at[slot, :, part(h)],
            rs_s.at[slot, h], rs_r.at[slot, h], (sp, to),
        )

    def give(i):
        b = turn_order[i]
        slot = jnp.where(b == flip3, DIAG, VIA)
        for h in (0, 1):

            @pl.when((b == flip3) | (b == lead[h]))
            def _():
                given(slot, h, b, lead[h]).start()

    def give_on(h):
        given(DIAG, h, 0, lead[h]).wait_recv()
        b = lead[1 - h]
        proj[b, :, part(h)] = (
            proj[b, :, part(h)].astype(f32) + rs_in[DIAG, :, part(h)].astype(f32)
        ).astype(bf)
        c = given(ON, h, b, b)
        c.start()
        sent.append(c)

    def rim_in(now):
        @pl.when(now & (sp > 0))
        def _():
            for c in rims:
                c.wait_recv()

        @pl.when(now & (sp == 0))
        def _():
            rim[...] = jnp.zeros(rim.shape, bf)

        @pl.when(now)
        def _():
            fill(rim.at[0], rim.at[1], 0)

    def slots():
        def mine(x):
            x = jnp.broadcast_to(x, (8, x.shape[1]))
            x = jnp.where(t >= 2, x[:, LANES:], x[:, :LANES])
            return jnp.where(lax.rem(t, 2) == 1, pltpu.roll(x, row_n, 1), x)

        picks = [mine(ids[k : k + 1, :]) for k in (0, 1)]
        parts = [mine(weights[k : k + 1, :]) for k in (0, 1)]
        lane = lax.broadcasted_iota(jnp.int32, (8, LANES), 1)
        sub = lax.broadcasted_iota(jnp.int32, (8, LANES), 0)
        group = jnp.where(lane < row_n, picks[0] // 2, -1)
        hit = sub == group
        before = (spot < lane_i).astype(bf)
        rank = jnp.dot(hit.astype(f32).astype(bf), before, preferred_element_type=f32)
        rank = jnp.sum(jnp.where(hit, rank, 0.0), 0, keepdims=True).astype(jnp.int32)
        slot = group[0:1] * cap + rank
        slot = jnp.where(lane[0:1] < row_n, slot, -1)
        chosen = (spot == jnp.broadcast_to(slot, (LANES, LANES))).astype(f32).astype(bf)
        sel[0] = chosen
        sel[1] = lax.dot_general(
            (spot == lane_i).astype(f32).astype(bf), chosen, (((1,), (1,)), ((), ())),
            preferred_element_type=f32,
        ).astype(bf)
        table = jnp.zeros((8, LANES), f32)
        for p in (0, 1):
            w = sum(jnp.where(lax.rem(picks[k], 2) == p, parts[k], 0.0) for k in (0, 1))
            w = jnp.where(lane < row_n, w, 0.0)
            high = w.astype(bf).astype(f32)
            table = jnp.where(sub == p, high, table)
            table = jnp.where(sub == p + 2, w - high, table)
        table = jnp.concatenate([table, jnp.zeros((LANES - 8, LANES), f32)], 0).astype(bf)
        ext[...] = lax.dot_general(
            chosen, table, (((1,), (1,)), ((), ())), preferred_element_type=f32
        ).astype(bf)

    def meet():
        pl.semaphore_wait(barrier, len(friends))

    def gathered():
        for h in (0, 1):
            given(VIA, h, 0, lead[h]).wait_recv()
            given(ON, h, 0, lead[1 - h]).wait_recv()

    ask()
    slots()
    meet()
    rim_out()
    fill_own()
    attend_block(0)
    give(0)
    rim_in(upper)
    attend_block(1)
    give(1)
    rim_in(t < tp_n // 2)
    attend_block(2)
    give(2)
    attend_block(3)
    give(3)
    give_on(0)
    give_on(1)
    gathered()
    for c in feeds[-2:]:
        c.wait()
    total = resid[...].astype(f32) + (
        proj[t].astype(f32) + rs_in[VIA].astype(f32) + rs_in[ON].astype(f32)
    )
    middle = total.astype(bf)
    mid[...] = middle
    mf = middle.astype(f32)
    scale = lax.rsqrt(jnp.mean(mf * mf, -1, keepdims=True) + norm_epsilon)
    normed[...] = (mf * scale * gain[...]).astype(bf)

    def block(tt, cc, zz):
        return rows.at[zz, pl.ds(pl.multiple_of((cc * tp_n + tt) * cap, cap), cap)]

    def pack(g, ref):
        spots = pl.ds(pl.multiple_of(g * cap, cap), cap)
        ref[:, :width] = jnp.dot(
            sel[0, spots, :row_n], normed[...], preferred_element_type=f32
        ).astype(bf)
        ref[:, width:] = ext[spots, :]

    ag = {}
    pt = {}
    swap = {}
    r2 = {}
    disp = {}
    bk = []

    def push(d, i, tt, to):
        ref = block(tt, core, plane[i])
        ag[(d, i)] = send(ref, ref, ag_s.at[d, i], ag_r.at[d, i], (sp, to))

    def across(d, i, tt):
        ref = block(tt, core, plane[i])
        pt[(d, i)] = send(ref, ref, pt_s.at[d, i], pt_r.at[d, i], (partner, t))

    def dispatch(i):
        g = plane[i]
        pack(g, outb.at[i])
        disp[i] = send(outb.at[i], block(t, core, z), di_s.at[i], di_r.at[i], (2 * g + core, t))

    def spread(i):
        if i:
            disp[i].wait_recv()
        push(VIA, i, t, via_t)
        push(ON, i, t, on_t)
        across(3, i, t)

    def relay(i):
        ag[(VIA, i)].wait_recv()
        push(DIAG, i, via_t, on_t)
        across(VIA, i, via_t)

    def other(i):
        ag[(ON, i)].wait_recv()
        across(ON, i, on_t)

    def corner(i):
        ag[(DIAG, i)].wait_recv()
        across(DIAG, i, flip3)

    def widen(i, h):
        if h == 0:
            for d in range(4):
                pt[(d, i)].wait_recv()
        if i == 0 and h == 0:
            for c in loads[1:]:
                c.wait()
        size = wg.shape[1] // PIECES
        cols = pl.ds(h * size, size)
        x = rows[plane[i], :, :width]
        g = jnp.dot(x, wg[:, cols], preferred_element_type=jnp.float32)
        u = jnp.dot(x, wu[:, cols], preferred_element_type=jnp.float32)
        hid[i, :, cols] = (g / (1.0 + jnp.exp(-g)) * u).astype(jnp.bfloat16)

    def part_cols(i, h):
        size = width // PIECES
        return pl.ds(h * size, size)

    def narrow(i, h):
        ext = rows[plane[i], :, width:].astype(jnp.float32)
        lane = lax.broadcasted_iota(jnp.int32, ext.shape, 1)
        mine = (lane == core) | (lane == core + 2)
        weight = jnp.sum(jnp.where(mine, ext, 0.0), -1, keepdims=True)
        tiles = width // TILE // PIECES

        @pl.loop(h * tiles, (h + 1) * tiles)
        def _(n):
            cols = pl.ds(pl.multiple_of(n * TILE, TILE), TILE)
            y = jnp.dot(hid[i], wd[:, cols], preferred_element_type=jnp.float32)
            outp[i, :, cols] = (y * weight).astype(jnp.bfloat16)

        here = part_cols(i, h)
        other_half = outp.at[i, pl.ds(pl.multiple_of((1 - core) * half, half), half), here]
        swap[(i, h)] = send(
            other_half, pr.at[i, :, here], pr_s.at[i, h], pr_r.at[i, h], (partner, t)
        )

    def own(i, h, tt):
        here = part_cols(i, h)
        mine = pl.ds(pl.multiple_of((core * tp_n + tt) * cap, cap), cap)
        theirs = pl.ds(pl.multiple_of(tt * cap, cap), cap)
        return outp[i, mine, here].astype(jnp.float32) + pr[i, theirs, here].astype(jnp.float32)

    def ship(d, i, h, to):
        here = part_cols(i, h)
        r2[(d, i, h)] = send(
            comb.at[i, d, :, here], rs2.at[i, d, :, here],
            r2_s.at[d, i, h], r2_r.at[d, i, h], (sp, to),
        )

    def combine(i, h):
        here = part_cols(i, h)
        swap[(i, h)].wait_recv()
        comb[i, DIAG, :, here] = own(i, h, flip3).astype(jnp.bfloat16)
        ship(DIAG, i, h, via_t)
        comb[i, VIA, :, here] = own(i, h, via_t).astype(jnp.bfloat16)
        ship(VIA, i, h, via_t)

    def combine_on(i, h):
        here = part_cols(i, h)
        r2[(DIAG, i, h)].wait_recv()
        comb[i, ON, :, here] = (
            own(i, h, on_t) + rs2[i, DIAG, :, here].astype(jnp.float32)
        ).astype(jnp.bfloat16)
        ship(ON, i, h, on_t)

    def finish(i, h):
        here = part_cols(i, h)
        acc = own(i, h, t)
        for d in (VIA, ON):
            r2[(d, i, h)].wait_recv()
            acc = acc + rs2[i, d, :, here].astype(jnp.float32)
        if i:
            ret[i, :, here] = acc.astype(jnp.bfloat16)
            bk.append(
                send(
                    ret.at[i, :, here], back.at[z, :, here], bk_s.at[i, h], bk_r.at[i, h],
                    (2 * plane[i] + core, t),
                )
            )
        else:
            back[z, :, here] = acc.astype(jnp.bfloat16)

    pack(z, block(t, core, z))
    spread(0)
    dispatch(1)
    dispatch(2)
    dispatch(3)
    relay(0)
    other(0)
    spread(1)
    spread(2)
    corner(0)
    relay(1)
    widen(0, 0)
    other(1)
    widen(0, 1)
    relay(2)
    spread(3)
    narrow(0, 0)
    corner(1)
    other(2)
    narrow(0, 1)
    widen(1, 0)
    combine(0, 0)
    widen(1, 1)
    corner(2)
    narrow(1, 0)
    relay(3)
    widen(2, 0)
    widen(2, 1)
    combine(1, 0)
    other(3)
    narrow(2, 0)
    combine(0, 1)
    corner(3)
    narrow(2, 1)
    combine(2, 0)
    widen(3, 0)
    combine_on(1, 0)
    combine(2, 1)
    widen(3, 1)
    narrow(3, 0)
    combine_on(2, 0)
    narrow(3, 1)
    combine(3, 0)
    finish(1, 0)
    narrow(1, 1)
    combine(3, 1)
    combine(1, 1)
    finish(2, 0)
    combine_on(3, 0)
    combine_on(3, 1)
    combine_on(2, 1)
    combine_on(1, 1)
    finish(3, 0)
    finish(3, 1)
    combine_on(0, 0)
    finish(2, 1)
    finish(1, 1)
    combine_on(0, 1)
    finish(0, 0)
    finish(0, 1)
    for c in bk:
        c.wait_recv()
    routed = jnp.dot(
        sel[1, :row_n, :], back[...].reshape(half, width), preferred_element_type=f32
    )
    out[...] = mid[...].astype(f32) + routed
    for c in sent:
        c.wait_send()
    for h in (0, 1):
        for slot in (VIA, DIAG):
            given(slot, h, 0, lead[h]).wait_send()

    @pl.when(sp < sp_n - 1)
    def _():
        for c in rims:
            c.wait_send()


def group_layer(
    queries, key_rows, values, sink_logits, residual, out_weight, norm_gain, expert_ids,
    route_weight, gate, up, down,
):
    row_n, width = residual.shape
    local = queries.shape[0]
    tp_n = lax.axis_size("tp")
    expert_n = lax.axis_size("sp")
    cap = 2 * max(1, 2 * row_n // expert_n)
    ext_width = width + LANES
    ff = gate.shape[-1]
    half = GROUPS * cap
    kv_heads = key_rows.shape[1] // HEAD
    frequency = 10000.0 ** (-(np.arange(LANES) % (HEAD // 2)) * 2.0 / HEAD)
    sign = np.where(np.arange(LANES) % HEAD < HEAD // 2, -1.0, 1.0)

    def turns(positions):
        angle = positions[:, None] * frequency[None, :]
        return jnp.asarray(
            np.concatenate([np.cos(angle), np.sin(angle) * sign], 1), jnp.float32
        )

    turn_row = turns(np.arange(local + WINDOW) - float(WINDOW))
    turn_base = turns(np.arange(expert_n) * float(local))
    bf = jnp.bfloat16
    dma = pltpu.SemaphoreType.DMA
    vmem = pl.BlockSpec(memory_space=pltpu.VMEM)
    hbm = pl.BlockSpec(memory_space=pltpu.HBM)
    total = pl.pallas_call(
        group_kernel,
        out_shape=jax.ShapeDtypeStruct((row_n, width), jnp.float32),
        in_specs=[hbm] * 14,
        out_specs=vmem,
        scratch_shapes=[
            pltpu.SMEM(sink_logits.shape, jnp.float32),
            pltpu.VMEM(queries.shape, bf),
            pltpu.VMEM(key_rows.shape, bf),
            pltpu.VMEM(values.shape, bf),
            pltpu.VMEM(turn_row.shape, jnp.float32),
            pltpu.VMEM(turn_base.shape, jnp.float32),
            pltpu.VMEM(residual.shape, bf),
            pltpu.VMEM((1, width), jnp.float32),
            pltpu.VMEM(expert_ids.shape[::-1], jnp.int32),
            pltpu.VMEM(route_weight.shape[::-1], jnp.float32),
            dma((10,)),
            pltpu.VMEM(out_weight.shape, bf),
            pltpu.VMEM((width, ff), bf),
            pltpu.VMEM((width, ff), bf),
            pltpu.VMEM((ff, width), bf),
            dma((4,)),
            pltpu.VMEM((2, WINDOW, key_rows.shape[1]), bf),
            dma((2,)),
            dma((2,)),
            pltpu.VMEM((tp_n, queries.shape[1] // LANES, 2 * row_n, LANES), bf),
            pltpu.VMEM((kv_heads, local + WINDOW + row_n, LANES), bf),
            pltpu.VMEM((kv_heads, local + WINDOW + row_n, LANES), bf),
            pltpu.VMEM((row_n, queries.shape[1]), bf),
            pltpu.VMEM((tp_n, row_n, width), bf),
            pltpu.VMEM((3, row_n, width), bf),
            dma((3, 2)),
            dma((3, 2)),
            pltpu.VMEM((2, LANES, LANES), bf),
            pltpu.VMEM((LANES, LANES), bf),
            pltpu.VMEM((row_n, width), bf),
            pltpu.VMEM((row_n, width), bf),
            pltpu.VMEM((GROUPS, cap, ext_width), bf),
            pltpu.VMEM((GROUPS, 2 * half, ext_width), bf),
            dma((GROUPS,)),
            dma((GROUPS,)),
            dma((3, GROUPS)),
            dma((3, GROUPS)),
            dma((4, GROUPS)),
            dma((4, GROUPS)),
            pltpu.VMEM((GROUPS, 2 * half, ff), bf),
            pltpu.VMEM((GROUPS, 2 * half, width), bf),
            pltpu.VMEM((GROUPS, half, width), bf),
            dma((GROUPS, 2)),
            dma((GROUPS, 2)),
            pltpu.VMEM((GROUPS, 3, cap, width), bf),
            pltpu.VMEM((GROUPS, 3, cap, width), bf),
            dma((3, GROUPS, 2)),
            dma((3, GROUPS, 2)),
            pltpu.VMEM((GROUPS, cap, width), bf),
            pltpu.VMEM((GROUPS, cap, width), bf),
            dma((GROUPS, 2)),
            dma((GROUPS, 2)),
        ],
        compiler_params=pltpu.CompilerParams(
            collective_id=0, has_side_effects=True, vmem_limit_bytes=50 * 2**20
        ),
    )(
        *(
            pltpu.with_memory_space_constraint(x, pltpu.HBM)
            for x in (
                sink_logits, queries, key_rows, values, turn_row, turn_base, residual,
                norm_gain[None], expert_ids.T, route_weight.T, out_weight, gate[0], up[0], down[0],
            )
        )
    )
    return total.astype(bf)


def per_device(
    queries,
    key_rows,
    values,
    sink_logits,
    residual,
    out_weight,
    norm_gain,
    expert_ids,
    route_weight,
    gate_proj,
    up_proj,
    down_proj,
):
    local_len = queries.shape[0]
    if lax.axis_size("tp") == 4 and lax.axis_size("sp") == 2 * GROUPS:
        return group_layer(
            queries, key_rows, values, sink_logits, residual, out_weight, norm_gain,
            expert_ids, route_weight, gate_proj, up_proj, down_proj,
        )
    q_heads = sink_logits.shape[0]
    kv_heads = key_rows.shape[1] // HEAD
    group_size = q_heads // kv_heads
    window_len = WINDOW
    seq_start = lax.axis_index("sp") * local_len
    rim_pair = jnp.stack([key_rows[local_len - window_len :], values[local_len - window_len :]])
    rim_pair = from_behind(rim_pair, "sp", 1)
    key_ext = jnp.concatenate([rim_pair[0], key_rows], 0)
    val_ext = jnp.concatenate([rim_pair[1], values], 0)
    positions = seq_start + jnp.arange(local_len, dtype=jnp.int32)
    ext_positions = seq_start - window_len + jnp.arange(local_len + window_len, dtype=jnp.int32)
    rot_query = rotary(queries, positions, q_heads)
    rot_key = rotary(key_ext, ext_positions, kv_heads)
    block_count = local_len // window_len
    query_blocks = rot_query.reshape(block_count, window_len, kv_heads, group_size, HEAD)
    key_blocks = rot_key.reshape(block_count + 1, window_len, kv_heads, HEAD)
    value_blocks = val_ext.reshape(block_count + 1, window_len, kv_heads, HEAD)
    key_pairs = jnp.concatenate([key_blocks[:-1], key_blocks[1:]], 1)
    value_pairs = jnp.concatenate([value_blocks[:-1], value_blocks[1:]], 1)
    sink_grid = sink_logits.reshape(kv_heads, group_size)
    attended = attend(query_blocks, key_pairs, value_pairs, sink_grid, seq_start - window_len)
    tok_rows = residual.shape[0]
    tp_count = lax.axis_size("tp")
    tp_index = lax.axis_index("tp")
    projected = lax.psum_scatter(
        jnp.dot(attended, out_weight, preferred_element_type=jnp.float32).astype(jnp.bfloat16),
        "tp",
        scatter_dimension=0,
        tiled=True,
    ).astype(jnp.float32)
    middle = (residual.astype(jnp.float32) + projected).astype(jnp.bfloat16)
    middle_f = middle.astype(jnp.float32)
    normed = (
        middle_f
        * lax.rsqrt(jnp.mean(middle_f * middle_f, -1, keepdims=True) + norm_epsilon)
        * norm_gain
    ).astype(jnp.bfloat16)
    expert_count = lax.axis_size("sp")
    capacity = 2 * max(1, 2 * tok_rows // expert_count)
    model_width = normed.shape[1]
    own_ids = lax.dynamic_slice_in_dim(expert_ids, tp_index * tok_rows, tok_rows, 0)
    own_weights = lax.dynamic_slice_in_dim(route_weight, tp_index * tok_rows, tok_rows, 0)
    select = slot_select(own_ids, expert_count, capacity)
    token_select = jnp.sum(select.reshape(expert_count * capacity, tok_rows, 2), -1)
    outbound = jnp.dot(token_select, normed, preferred_element_type=jnp.float32).astype(
        jnp.bfloat16
    )
    outbound = outbound.reshape(expert_count, capacity, model_width)
    arrived = lax.all_to_all(outbound, "sp", split_axis=0, concat_axis=0, tiled=True)
    partial_out = expert_part(
        lax.all_gather(arrived, "tp", axis=0, tiled=True), gate_proj, up_proj, down_proj
    )
    partial_out = partial_out.reshape(tp_count, expert_count * capacity, model_width)
    width_parts = lax.all_to_all(partial_out, "tp", split_axis=0, concat_axis=0, tiled=True)
    summed = jnp.sum(width_parts.astype(jnp.float32), 0).reshape(
        expert_count, capacity, model_width
    )
    returned = (
        lax.all_to_all(summed.astype(jnp.bfloat16), "sp", split_axis=0, concat_axis=0, tiled=True)
        .astype(summed.dtype)
        .reshape(expert_count * capacity, model_width)
    )
    picked = jnp.dot(
        select.astype(jnp.float32).T,
        returned,
        precision=lax.Precision.HIGHEST,
        preferred_element_type=jnp.float32,
    )
    routed = jnp.sum(picked.reshape(tok_rows, 2, model_width) * own_weights[..., None], 1)
    return (middle_f + routed).astype(jnp.bfloat16)


def solution(mesh):
    return jax.shard_map(
        per_device,
        mesh=mesh,
        in_specs=(
            P("sp", "tp"),
            P("sp", "tp"),
            P("sp", "tp"),
            P("tp"),
            P(("sp", "tp"), None),
            P("tp", None),
            P(),
            P("sp", None),
            P("sp", None),
            P("sp", None, "tp"),
            P("sp", None, "tp"),
            P("sp", "tp", None),
        ),
        out_specs=P(("sp", "tp"), None),
        check_vma=False,
    )
```

```python
import jax
import jax.numpy as jnp
import numpy as np
from jax import lax
from jax.experimental import pallas as pl
from jax.experimental.pallas import tpu as pltpu
from jax.sharding import PartitionSpec as P

HEAD = 64
WINDOW = 128


norm_epsilon = 1e-06


def from_behind(block, axis, distance):
    devices = range(lax.axis_size(axis))
    route = [(i - distance, i) for i in devices if i - distance in devices]
    return lax.ppermute(block, axis, route)


def rotary(values_in, positions, head_count):
    halfway = HEAD // 2
    frequency = 10000.0 ** (-jnp.arange(halfway, dtype=jnp.float32) * 2.0 / HEAD)
    angles = positions.astype(jnp.float32)[:, None] * frequency[None, :]
    cosine = jnp.cos(angles)[:, None, :]
    sine_part = jnp.sin(angles)[:, None, :]
    reshaped = values_in.astype(jnp.float32).reshape(values_in.shape[0], head_count, HEAD)
    front_part = reshaped[..., :halfway]
    back_part = reshaped[..., halfway:]
    turned = jnp.concatenate(
        [front_part * cosine - back_part * sine_part, back_part * cosine + front_part * sine_part],
        -1,
    )
    return turned.astype(jnp.bfloat16)


def attend(query_blocks, key_pairs, value_pairs, sink_grid, key_start):
    block_count = query_blocks.shape[0]
    window_len = query_blocks.shape[1]
    scores = jnp.einsum(
        "bqkgd,bskd->bkgqs", query_blocks, key_pairs, preferred_element_type=jnp.float32
    ) * HEAD ** (-0.5)
    row_idx = jnp.arange(window_len)[:, None]
    col_idx = jnp.arange(2 * window_len)[None, :]
    distance = row_idx - col_idx + window_len
    key_pos = key_start + jnp.arange(block_count)[:, None, None] * window_len + col_idx[None]
    allowed = (distance >= 0)[None] & (distance < window_len)[None] & (key_pos >= 0)
    scores = jnp.where(allowed[:, None, None], scores, -jnp.inf)
    sink_full = sink_grid[None, :, :, None]
    highest = jnp.maximum(jnp.max(scores, -1), sink_full)
    exp_scores = jnp.exp(scores - highest[..., None])
    denominator = jnp.sum(exp_scores, -1) + jnp.exp(sink_full - highest)
    weighted = jnp.einsum(
        "bkgqs,bskd->bkgqd",
        exp_scores.astype(jnp.bfloat16),
        value_pairs,
        preferred_element_type=jnp.float32,
    )
    normalized = weighted / denominator[..., None]
    return (
        jnp.transpose(normalized, (0, 3, 1, 2, 4))
        .astype(jnp.bfloat16)
        .reshape(block_count * window_len, -1)
    )


def slot_select(picks_in, expert_count, capacity):
    flattened = picks_in.reshape(-1)
    onehot = (flattened[:, None] == jnp.arange(expert_count, dtype=jnp.int32)[None, :]).astype(
        jnp.int32
    )
    rank_of = jnp.sum(jnp.cumsum(onehot, 0) * onehot, 1) - 1
    slot_of = flattened * capacity + rank_of
    chosen = jnp.arange(expert_count * capacity, dtype=jnp.int32)[:, None] == slot_of[None, :]
    return chosen.astype(jnp.bfloat16)


def expert_part(rows_in, gate_proj, up_proj, down_proj):
    in_shape = rows_in.shape
    flattened = rows_in.reshape(-1, in_shape[-1])
    gate_val = jnp.dot(flattened, gate_proj[0], preferred_element_type=jnp.float32)
    up_val = jnp.dot(flattened, up_proj[0], preferred_element_type=jnp.float32)
    hidden = (jax.nn.silu(gate_val) * up_val).astype(jnp.bfloat16)
    return (
        jnp.dot(hidden, down_proj[0], preferred_element_type=jnp.float32)
        .astype(jnp.bfloat16)
        .reshape(in_shape)
    )


GROUPS = 4
LANES = 128
MESH = pl.DeviceIdType.MESH
VIA, ON, DIAG = 0, 1, 2


PIECES = 2


def group_kernel(
    sink_hbm, q_hbm, k_hbm, v_hbm, row_hbm, base_hbm, resid_hbm, gain_hbm, ids_hbm, weights_hbm,
    wo_hbm, wg_hbm, wu_hbm, wd_hbm, out,
    sink, q_in, k_in, v_in, turn_row, turn_base, resid, gain, ids, weights, in_sem,
    wo, wg, wu, wd, w_sem,
    rim, rim_s, rim_r, asks, keys, vals, att,
    proj, rs_in, rs_s, rs_r,
    sel, ext,
    mid, normed, outb, rows,
    di_s, di_r, ag_s, ag_r, pt_s, pt_r,
    hid, outp, pr, pr_s, pr_r,
    comb, rs2, r2_s, r2_r,
    ret, back, bk_s, bk_r,
):
    sp = lax.axis_index("sp")
    t = lax.axis_index("tp")
    sp_n = lax.axis_size("sp")
    core = lax.rem(sp, 2)
    z = sp // 2
    tp_n, row_n, width = proj.shape
    cap = outb.shape[1]
    half = GROUPS * cap
    flip1 = t + 1 - 2 * lax.rem(t, 2)
    flip2 = lax.rem(t + 2, 4)
    flip3 = lax.rem(flip1 + 2, 4)
    peer = [t, flip1, flip2, flip3]
    via_t = flip1 + core * (flip2 - flip1)
    on_t = flip2 + core * (flip1 - flip2)
    partner = sp + 1 - 2 * core
    plane = [z, z + 1 - 2 * lax.rem(z, 2), lax.rem(z + 2, GROUPS), GROUPS - 1 - z]

    barrier = pltpu.get_barrier_semaphore()
    rim_peer = lax.rem(sp + 2 * core - 1 + sp_n, sp_n)
    friends = [(sp, peer[d]) for d in (1, 2, 3)]
    friends += [(plane[i] * 2 + core, t) for i in (1, 2, 3)] + [(partner, t), (rim_peer, t)]
    for dev in friends:
        pl.semaphore_signal(barrier, inc=1, device_id=dev, device_id_type=MESH)

    moves = (
        (row_hbm, turn_row), (base_hbm, turn_base), (q_hbm, q_in), (k_hbm, k_in), (v_hbm, v_in),
        (ids_hbm, ids), (weights_hbm, weights), (sink_hbm, sink),
        (resid_hbm, resid), (gain_hbm, gain),
    )
    feeds = [pltpu.make_async_copy(a, b, in_sem.at[i]) for i, (a, b) in enumerate(moves)]
    loads = [
        pltpu.make_async_copy(a, b, w_sem.at[i])
        for i, (a, b) in enumerate(((wo_hbm, wo), (wg_hbm, wg), (wu_hbm, wu), (wd_hbm, wd)))
    ]
    for c in feeds + loads:
        c.start()

    sent = []

    def describe(src, dst, ss, rs, dev):
        return pltpu.make_async_remote_copy(
            src_ref=src, dst_ref=dst, send_sem=ss, recv_sem=rs, device_id=dev, device_id_type=MESH
        )

    def send(src, dst, ss, rs, dev):
        c = describe(src, dst, ss, rs, dev)
        c.start()
        sent.append(c)
        return c

    bf = jnp.bfloat16
    f32 = jnp.float32
    local = q_in.shape[0]
    tiles = k_in.shape[1] // LANES
    pairs = q_in.shape[1] // LANES
    edge = WINDOW
    pad = keys.shape[1] - local - edge
    span = pad + edge + row_n

    for c in feeds[:-2]:
        c.wait()
    at_sp = lax.broadcasted_iota(jnp.int32, turn_base.shape, 0) == sp
    start = jnp.sum(jnp.where(at_sp, turn_base[...], 0.0), 0, keepdims=True)
    cb, sb = start[:, :LANES], start[:, LANES:]
    cr = turn_row[:, :LANES]
    sr = turn_row[:, LANES:]
    cosine = cb * cr - sb * sr
    sine = sb * cr + cb * sr
    spot = lax.broadcasted_iota(jnp.int32, (LANES, LANES), 0)
    lane_i = lax.broadcasted_iota(jnp.int32, (LANES, LANES), 1)
    swapped = jnp.where(lax.rem(lane_i, HEAD) < HEAD // 2, lane_i + HEAD // 2, lane_i - HEAD // 2)
    exchange = (spot == swapped).astype(bf)

    def turned(x, lo):
        n = x.shape[0]
        y = jnp.dot(x, exchange, preferred_element_type=f32)
        return x.astype(f32) * cosine[lo : lo + n] + y * sine[lo : lo + n]

    def doubled(x, ref, j, lo):
        n = x.shape[0]
        moved = pltpu.roll(x, HEAD, 1)
        first = lax.broadcasted_iota(jnp.int32, x.shape, 1) < HEAD
        ref[2 * j, lo : lo + n, :] = jnp.where(first, x, moved).astype(bf)
        ref[2 * j + 1, lo : lo + n, :] = jnp.where(first, moved, x).astype(bf)

    rim_next = lax.rem(sp + 1, sp_n)
    rims = [
        describe(
            src.at[pl.ds(local - edge, edge)], rim.at[i], rim_s.at[i], rim_r.at[i], (rim_next, t)
        )
        for i, src in enumerate((k_in, v_in))
    ]

    def rim_out():
        @pl.when(sp < sp_n - 1)
        def _():
            for c in rims:
                c.start()

    def fill(k_src, v_src, lo):
        for j in range(tiles):
            cols = slice(j * LANES, (j + 1) * LANES)
            doubled(turned(k_src[:, cols], lo), keys, j, lo + pad)
            doubled(v_src[:, cols].astype(f32), vals, j, lo + pad)

    def ask():
        lane = lax.broadcasted_iota(jnp.int32, (local, LANES), 1)
        for j in range(pairs):
            q = turned(q_in[:, j * LANES : (j + 1) * LANES], edge) * HEAD ** (-0.5)
            head = [jnp.where(lane < HEAD, q, 0.0), jnp.where(lane < HEAD, 0.0, q)]
            for i in (0, 1):
                for b in range(tp_n):
                    asks[b, j, i * row_n : (i + 1) * row_n, :] = head[i][
                        b * row_n : (b + 1) * row_n
                    ].astype(bf)
        keys[:, :pad, :] = jnp.zeros((keys.shape[0], pad, LANES), bf)
        vals[:, :pad, :] = jnp.zeros((keys.shape[0], pad, LANES), bf)

    def fill_own():
        fill(k_in, v_in, edge)

    upper = t >= tp_n // 2
    turn_order = [
        jnp.where(upper, t, flip3),
        jnp.where(upper, flip3, flip2),
        flip1,
        jnp.where(upper, flip2, t),
    ]

    def attend_block(i):
        b = turn_order[i]
        start_at = pl.multiple_of(b * row_n, row_n)
        shape = (2 * row_n, span)
        row = lax.rem(lax.broadcasted_iota(jnp.int32, shape, 0), row_n)
        col = lax.broadcasted_iota(jnp.int32, shape, 1)
        ahead = col - row
        key_pos = sp * local + b * row_n - pad - edge + col
        allowed = (ahead > pad + edge - WINDOW) & (ahead <= pad + edge) & (key_pos >= 0)
        lane = lax.broadcasted_iota(jnp.int32, (row_n, LANES), 1)
        top = lax.broadcasted_iota(jnp.int32, (2 * row_n, 1), 0) < row_n
        window = pl.ds(start_at, span)
        all_j = range(pairs)
        scores = [
            lax.dot_general(
                asks[b, j], keys[j, window, :], (((1,), (1,)), ((), ())),
                preferred_element_type=f32,
            )
            for j in all_j
        ]
        scores = [jnp.where(allowed, s, -jnp.inf) for s in scores]
        rest = [jnp.where(top, sink[2 * j], sink[2 * j + 1]) for j in all_j]
        highest = [
            jnp.maximum(jnp.max(scores[j], -1, keepdims=True), rest[j]) for j in all_j
        ]
        probs = [jnp.exp(scores[j] - highest[j]) for j in all_j]
        mixed = [
            jnp.dot(probs[j].astype(bf), vals[j, window, :], preferred_element_type=f32)
            for j in all_j
        ]
        share = [
            1.0 / (jnp.sum(probs[j], -1, keepdims=True) + jnp.exp(rest[j] - highest[j]))
            for j in all_j
        ]
        for j in all_j:
            m = mixed[j] * share[j]
            att[:, j * LANES : (j + 1) * LANES] = jnp.where(
                lane < HEAD, m[:row_n], m[row_n:]
            ).astype(bf)
        if i == 0:
            loads[0].wait()
        proj[b] = jnp.dot(att[...], wo[...], preferred_element_type=f32).astype(bf)

    lead = [via_t, on_t]

    def part(h):
        size = width // 2
        return slice(h * size, (h + 1) * size)

    def given(slot, h, b, to):
        return describe(
            proj.at[b, :, part(h)], rs_in.at[slot, :, part(h)],
            rs_s.at[slot, h], rs_r.at[slot, h], (sp, to),
        )

    def give(i):
        b = turn_order[i]
        slot = jnp.where(b == flip3, DIAG, VIA)
        for h in (0, 1):

            @pl.when((b == flip3) | (b == lead[h]))
            def _():
                given(slot, h, b, lead[h]).start()

    def give_on(h):
        given(DIAG, h, 0, lead[h]).wait_recv()
        b = lead[1 - h]
        proj[b, :, part(h)] = (
            proj[b, :, part(h)].astype(f32) + rs_in[DIAG, :, part(h)].astype(f32)
        ).astype(bf)
        c = given(ON, h, b, b)
        c.start()
        sent.append(c)

    def rim_in(now):
        @pl.when(now & (sp > 0))
        def _():
            for c in rims:
                c.wait_recv()

        @pl.when(now & (sp == 0))
        def _():
            rim[...] = jnp.zeros(rim.shape, bf)

        @pl.when(now)
        def _():
            fill(rim.at[0], rim.at[1], 0)

    def slots():
        def mine(x):
            x = jnp.broadcast_to(x, (8, x.shape[1]))
            x = jnp.where(t >= 2, x[:, LANES:], x[:, :LANES])
            return jnp.where(lax.rem(t, 2) == 1, pltpu.roll(x, row_n, 1), x)

        picks = [mine(ids[k : k + 1, :]) for k in (0, 1)]
        parts = [mine(weights[k : k + 1, :]) for k in (0, 1)]
        lane = lax.broadcasted_iota(jnp.int32, (8, LANES), 1)
        sub = lax.broadcasted_iota(jnp.int32, (8, LANES), 0)
        group = jnp.where(lane < row_n, picks[0] // 2, -1)
        hit = sub == group
        before = (spot < lane_i).astype(bf)
        rank = jnp.dot(hit.astype(f32).astype(bf), before, preferred_element_type=f32)
        rank = jnp.sum(jnp.where(hit, rank, 0.0), 0, keepdims=True).astype(jnp.int32)
        slot = group[0:1] * cap + rank
        slot = jnp.where(lane[0:1] < row_n, slot, -1)
        chosen = (spot == jnp.broadcast_to(slot, (LANES, LANES))).astype(f32).astype(bf)
        sel[0] = chosen
        sel[1] = lax.dot_general(
            (spot == lane_i).astype(f32).astype(bf), chosen, (((1,), (1,)), ((), ())),
            preferred_element_type=f32,
        ).astype(bf)
        table = jnp.zeros((8, LANES), f32)
        for p in (0, 1):
            w = sum(jnp.where(lax.rem(picks[k], 2) == p, parts[k], 0.0) for k in (0, 1))
            w = jnp.where(lane < row_n, w, 0.0)
            high = w.astype(bf).astype(f32)
            table = jnp.where(sub == p, high, table)
            table = jnp.where(sub == p + 2, w - high, table)
        table = jnp.concatenate([table, jnp.zeros((LANES - 8, LANES), f32)], 0).astype(bf)
        ext[...] = lax.dot_general(
            chosen, table, (((1,), (1,)), ((), ())), preferred_element_type=f32
        ).astype(bf)

    def meet():
        pl.semaphore_wait(barrier, len(friends))

    def gathered():
        for h in (0, 1):
            given(VIA, h, 0, lead[h]).wait_recv()
            given(ON, h, 0, lead[1 - h]).wait_recv()

    ask()
    fill_own()
    meet()
    rim_out()
    attend_block(0)
    give(0)
    rim_in(upper)
    attend_block(1)
    give(1)
    rim_in(t < tp_n // 2)
    attend_block(2)
    give(2)
    attend_block(3)
    give(3)
    slots()
    give_on(0)
    give_on(1)
    gathered()
    for c in feeds[-2:]:
        c.wait()
    total = resid[...].astype(f32) + (
        proj[t].astype(f32) + rs_in[VIA].astype(f32) + rs_in[ON].astype(f32)
    )
    middle = total.astype(bf)
    mid[...] = middle
    mf = middle.astype(f32)
    scale = lax.rsqrt(jnp.mean(mf * mf, -1, keepdims=True) + norm_epsilon)
    normed[...] = (mf * scale * gain[...]).astype(bf)

    def block(tt, cc, zz, g=None):
        first = pl.multiple_of((cc * tp_n + tt) * cap, cap)
        if g is None:
            return rows.at[zz, pl.ds(first, cap)]
        return rows.at[zz, pl.ds(pl.multiple_of(first + g * (cap // 2), cap // 2), cap // 2)]

    def pack(g, ref):
        spots = pl.ds(pl.multiple_of(g * cap, cap), cap)
        ref[:, :width] = jnp.dot(
            sel[0, spots, :row_n], normed[...], preferred_element_type=f32
        ).astype(bf)
        ref[:, width:] = ext[spots, :]

    ag = {}
    pt = {}
    swap = {}
    r2 = {}
    disp = {}
    bk = {}

    def push(step, g, half_i, i, tt, to):
        ref = block(tt, core, plane[i], half_i)
        n = 2 * step + g
        ag[(step, g, i)] = send(ref, ref, ag_s.at[n, i], ag_r.at[n, i], (sp, to))

    def across(d, i, tt):
        ref = block(tt, core, plane[i])
        pt[(d, i)] = send(ref, ref, pt_s.at[d, i], pt_r.at[d, i], (partner, t))

    def dispatch(i):
        g = plane[i]
        pack(g, outb.at[i])
        disp[i] = send(outb.at[i], block(t, core, z), di_s.at[i], di_r.at[i], (2 * g + core, t))

    def spread(i):
        if i:
            disp[i].wait_recv()
        for g in (0, 1):
            push(0, g, g, i, t, lead[g])
        for g in (0, 1):
            push(1, g, 1 - g, i, t, lead[g])
        across(3, i, t)

    def relay(i, g):
        ag[(0, g, i)].wait_recv()
        push(2, g, g, i, lead[g], lead[1 - g])

    def other(i):
        for g in (0, 1):
            ag[(1, g, i)].wait_recv()
            across(g, i, lead[g])

    def corner(i):
        for g in (0, 1):
            ag[(2, g, i)].wait_recv()
        across(2, i, flip3)

    def widen(i, h):
        if h == 0:
            for d in range(4):
                pt[(d, i)].wait_recv()
        if i == 0 and h == 0:
            for c in loads[1:]:
                c.wait()
        size = wg.shape[1] // PIECES
        cols = pl.ds(h * size, size)
        x = rows[plane[i], :, :width]
        g = jnp.dot(x, wg[:, cols], preferred_element_type=jnp.float32)
        u = jnp.dot(x, wu[:, cols], preferred_element_type=jnp.float32)
        hid[i, :, cols] = (g / (1.0 + jnp.exp(-g)) * u).astype(jnp.bfloat16)

    def part_cols(i, h):
        size = width // PIECES
        return pl.ds(h * size, size)

    def narrow(i, h):
        ext = rows[plane[i], :, width:].astype(jnp.float32)
        lane = lax.broadcasted_iota(jnp.int32, ext.shape, 1)
        mine = (lane == core) | (lane == core + 2)
        weight = jnp.sum(jnp.where(mine, ext, 0.0), -1, keepdims=True)
        cols = part_cols(i, h)
        y = jnp.dot(hid[i], wd[:, cols], preferred_element_type=jnp.float32)
        outp[i, :, cols] = (y * weight).astype(jnp.bfloat16)

        here = part_cols(i, h)
        other_half = outp.at[i, pl.ds(pl.multiple_of((1 - core) * half, half), half), here]
        swap[(i, h)] = send(
            other_half, pr.at[i, :, here], pr_s.at[i, h], pr_r.at[i, h], (partner, t)
        )

    def own(i, h, tt):
        here = part_cols(i, h)
        mine = pl.ds(pl.multiple_of((core * tp_n + tt) * cap, cap), cap)
        theirs = pl.ds(pl.multiple_of(tt * cap, cap), cap)
        return outp[i, mine, here].astype(jnp.float32) + pr[i, theirs, here].astype(jnp.float32)

    def ship(d, i, h, to):
        here = part_cols(i, h)
        r2[(d, i, h)] = send(
            comb.at[i, d, :, here], rs2.at[i, d, :, here],
            r2_s.at[d, i, h], r2_r.at[d, i, h], (sp, to),
        )

    def combine(i, h):
        here = part_cols(i, h)
        swap[(i, h)].wait_recv()
        comb[i, DIAG, :, here] = own(i, h, flip3).astype(jnp.bfloat16)
        ship(DIAG, i, h, lead[h])
        comb[i, VIA, :, here] = own(i, h, lead[h]).astype(jnp.bfloat16)
        ship(VIA, i, h, lead[h])

    def combine_on(i, h):
        here = part_cols(i, h)
        r2[(DIAG, i, h)].wait_recv()
        comb[i, ON, :, here] = (
            own(i, h, lead[1 - h]) + rs2[i, DIAG, :, here].astype(jnp.float32)
        ).astype(jnp.bfloat16)
        ship(ON, i, h, lead[1 - h])

    def finish(i, h):
        here = part_cols(i, h)
        acc = own(i, h, t)
        for d in (VIA, ON):
            r2[(d, i, h)].wait_recv()
            acc = acc + rs2[i, d, :, here].astype(jnp.float32)
        if i:
            ret[i, :, here] = acc.astype(jnp.bfloat16)
            bk[(i, h)] = describe(
                ret.at[i, :, here], back.at[z, :, here], bk_s.at[i, h], bk_r.at[i, h],
                (2 * plane[i] + core, t),
            )
            bk[(i, h)].start()
        else:
            back[z, :, here] = acc.astype(jnp.bfloat16)

    pack(z, block(t, core, z))
    spread(0)
    dispatch(1)
    dispatch(2)
    relay(0, 0)
    relay(0, 1)
    dispatch(3)
    spread(1)
    other(0)
    corner(0)
    relay(1, 0)
    relay(1, 1)
    spread(2)
    widen(0, 0)
    widen(0, 1)
    other(1)
    corner(1)
    relay(2, 0)
    relay(2, 1)
    narrow(0, 0)
    spread(3)
    widen(1, 0)
    other(2)
    widen(1, 1)
    corner(2)
    narrow(1, 0)
    relay(3, 0)
    relay(3, 1)
    widen(2, 0)
    combine(1, 0)
    other(3)
    widen(2, 1)
    narrow(2, 0)
    corner(3)
    narrow(2, 1)
    combine_on(1, 0)
    combine(2, 0)
    widen(3, 0)
    combine(2, 1)
    widen(3, 1)
    narrow(3, 0)
    combine_on(2, 0)
    narrow(1, 1)
    combine(3, 0)
    finish(1, 0)
    narrow(3, 1)
    combine_on(2, 1)
    finish(2, 0)
    combine(3, 1)
    combine_on(3, 0)
    combine(1, 1)
    finish(2, 1)
    combine_on(3, 1)
    combine(0, 0)
    finish(3, 0)
    narrow(0, 1)
    combine(0, 1)
    combine_on(1, 1)
    finish(3, 1)
    combine_on(0, 0)
    combine_on(0, 1)
    finish(1, 1)
    finish(0, 0)
    finish(0, 1)
    for c in sent:
        c.wait_send()
    for h in (0, 1):
        for slot in (VIA, DIAG):
            given(slot, h, 0, lead[h]).wait_send()

    @pl.when(sp < sp_n - 1)
    def _():
        for c in rims:
            c.wait_send()

    for h in range(PIECES):
        here = part_cols(0, h)
        for i in range(1, GROUPS):
            bk[(i, h)].wait_recv()
        routed = jnp.dot(
            sel[1, :row_n, :],
            back[:, :, here].reshape(half, width // PIECES),
            preferred_element_type=f32,
        )
        out[:, here] = mid[:, here].astype(f32) + routed
    for c in bk.values():
        c.wait_send()


def group_layer(
    queries, key_rows, values, sink_logits, residual, out_weight, norm_gain, expert_ids,
    route_weight, gate, up, down,
):
    row_n, width = residual.shape
    local = queries.shape[0]
    tp_n = lax.axis_size("tp")
    expert_n = lax.axis_size("sp")
    cap = 2 * max(1, 2 * row_n // expert_n)
    ext_width = width + LANES
    ff = gate.shape[-1]
    half = GROUPS * cap
    kv_heads = key_rows.shape[1] // HEAD
    frequency = 10000.0 ** (-(np.arange(LANES) % (HEAD // 2)) * 2.0 / HEAD)
    sign = np.where(np.arange(LANES) % HEAD < HEAD // 2, -1.0, 1.0)

    def turns(positions):
        angle = positions[:, None] * frequency[None, :]
        return jnp.asarray(
            np.concatenate([np.cos(angle), np.sin(angle) * sign], 1), jnp.float32
        )

    turn_row = turns(np.arange(local + WINDOW) - float(WINDOW))
    turn_base = turns(np.arange(expert_n) * float(local))
    bf = jnp.bfloat16
    dma = pltpu.SemaphoreType.DMA
    vmem = pl.BlockSpec(memory_space=pltpu.VMEM)
    hbm = pl.BlockSpec(memory_space=pltpu.HBM)
    total = pl.pallas_call(
        group_kernel,
        out_shape=jax.ShapeDtypeStruct((row_n, width), jnp.float32),
        in_specs=[hbm] * 14,
        out_specs=vmem,
        scratch_shapes=[
            pltpu.SMEM(sink_logits.shape, jnp.float32),
            pltpu.VMEM(queries.shape, bf),
            pltpu.VMEM(key_rows.shape, bf),
            pltpu.VMEM(values.shape, bf),
            pltpu.VMEM(turn_row.shape, jnp.float32),
            pltpu.VMEM(turn_base.shape, jnp.float32),
            pltpu.VMEM(residual.shape, bf),
            pltpu.VMEM((1, width), jnp.float32),
            pltpu.VMEM(expert_ids.shape[::-1], jnp.int32),
            pltpu.VMEM(route_weight.shape[::-1], jnp.float32),
            dma((10,)),
            pltpu.VMEM(out_weight.shape, bf),
            pltpu.VMEM((width, ff), bf),
            pltpu.VMEM((width, ff), bf),
            pltpu.VMEM((ff, width), bf),
            dma((4,)),
            pltpu.VMEM((2, WINDOW, key_rows.shape[1]), bf),
            dma((2,)),
            dma((2,)),
            pltpu.VMEM((tp_n, queries.shape[1] // LANES, 2 * row_n, LANES), bf),
            pltpu.VMEM((kv_heads, local + WINDOW + row_n, LANES), bf),
            pltpu.VMEM((kv_heads, local + WINDOW + row_n, LANES), bf),
            pltpu.VMEM((row_n, queries.shape[1]), bf),
            pltpu.VMEM((tp_n, row_n, width), bf),
            pltpu.VMEM((3, row_n, width), bf),
            dma((3, 2)),
            dma((3, 2)),
            pltpu.VMEM((2, LANES, LANES), bf),
            pltpu.VMEM((LANES, LANES), bf),
            pltpu.VMEM((row_n, width), bf),
            pltpu.VMEM((row_n, width), bf),
            pltpu.VMEM((GROUPS, cap, ext_width), bf),
            pltpu.VMEM((GROUPS, 2 * half, ext_width), bf),
            dma((GROUPS,)),
            dma((GROUPS,)),
            dma((6, GROUPS)),
            dma((6, GROUPS)),
            dma((4, GROUPS)),
            dma((4, GROUPS)),
            pltpu.VMEM((GROUPS, 2 * half, ff), bf),
            pltpu.VMEM((GROUPS, 2 * half, width), bf),
            pltpu.VMEM((GROUPS, half, width), bf),
            dma((GROUPS, 2)),
            dma((GROUPS, 2)),
            pltpu.VMEM((GROUPS, 3, cap, width), bf),
            pltpu.VMEM((GROUPS, 3, cap, width), bf),
            dma((3, GROUPS, 2)),
            dma((3, GROUPS, 2)),
            pltpu.VMEM((GROUPS, cap, width), bf),
            pltpu.VMEM((GROUPS, cap, width), bf),
            dma((GROUPS, 2)),
            dma((GROUPS, 2)),
        ],
        compiler_params=pltpu.CompilerParams(
            collective_id=0, has_side_effects=True, vmem_limit_bytes=50 * 2**20
        ),
    )(
        *(
            pltpu.with_memory_space_constraint(x, pltpu.HBM)
            for x in (
                sink_logits, queries, key_rows, values, turn_row, turn_base, residual,
                norm_gain[None], expert_ids.T, route_weight.T, out_weight, gate[0], up[0], down[0],
            )
        )
    )
    return total.astype(bf)


def per_device(
    queries,
    key_rows,
    values,
    sink_logits,
    residual,
    out_weight,
    norm_gain,
    expert_ids,
    route_weight,
    gate_proj,
    up_proj,
    down_proj,
):
    local_len = queries.shape[0]
    if lax.axis_size("tp") == 4 and lax.axis_size("sp") == 2 * GROUPS:
        return group_layer(
            queries, key_rows, values, sink_logits, residual, out_weight, norm_gain,
            expert_ids, route_weight, gate_proj, up_proj, down_proj,
        )
    q_heads = sink_logits.shape[0]
    kv_heads = key_rows.shape[1] // HEAD
    group_size = q_heads // kv_heads
    window_len = WINDOW
    seq_start = lax.axis_index("sp") * local_len
    rim_pair = jnp.stack([key_rows[local_len - window_len :], values[local_len - window_len :]])
    rim_pair = from_behind(rim_pair, "sp", 1)
    key_ext = jnp.concatenate([rim_pair[0], key_rows], 0)
    val_ext = jnp.concatenate([rim_pair[1], values], 0)
    positions = seq_start + jnp.arange(local_len, dtype=jnp.int32)
    ext_positions = seq_start - window_len + jnp.arange(local_len + window_len, dtype=jnp.int32)
    rot_query = rotary(queries, positions, q_heads)
    rot_key = rotary(key_ext, ext_positions, kv_heads)
    block_count = local_len // window_len
    query_blocks = rot_query.reshape(block_count, window_len, kv_heads, group_size, HEAD)
    key_blocks = rot_key.reshape(block_count + 1, window_len, kv_heads, HEAD)
    value_blocks = val_ext.reshape(block_count + 1, window_len, kv_heads, HEAD)
    key_pairs = jnp.concatenate([key_blocks[:-1], key_blocks[1:]], 1)
    value_pairs = jnp.concatenate([value_blocks[:-1], value_blocks[1:]], 1)
    sink_grid = sink_logits.reshape(kv_heads, group_size)
    attended = attend(query_blocks, key_pairs, value_pairs, sink_grid, seq_start - window_len)
    tok_rows = residual.shape[0]
    tp_count = lax.axis_size("tp")
    tp_index = lax.axis_index("tp")
    projected = lax.psum_scatter(
        jnp.dot(attended, out_weight, preferred_element_type=jnp.float32).astype(jnp.bfloat16),
        "tp",
        scatter_dimension=0,
        tiled=True,
    ).astype(jnp.float32)
    middle = (residual.astype(jnp.float32) + projected).astype(jnp.bfloat16)
    middle_f = middle.astype(jnp.float32)
    normed = (
        middle_f
        * lax.rsqrt(jnp.mean(middle_f * middle_f, -1, keepdims=True) + norm_epsilon)
        * norm_gain
    ).astype(jnp.bfloat16)
    expert_count = lax.axis_size("sp")
    capacity = 2 * max(1, 2 * tok_rows // expert_count)
    model_width = normed.shape[1]
    own_ids = lax.dynamic_slice_in_dim(expert_ids, tp_index * tok_rows, tok_rows, 0)
    own_weights = lax.dynamic_slice_in_dim(route_weight, tp_index * tok_rows, tok_rows, 0)
    select = slot_select(own_ids, expert_count, capacity)
    token_select = jnp.sum(select.reshape(expert_count * capacity, tok_rows, 2), -1)
    outbound = jnp.dot(token_select, normed, preferred_element_type=jnp.float32).astype(
        jnp.bfloat16
    )
    outbound = outbound.reshape(expert_count, capacity, model_width)
    arrived = lax.all_to_all(outbound, "sp", split_axis=0, concat_axis=0, tiled=True)
    partial_out = expert_part(
        lax.all_gather(arrived, "tp", axis=0, tiled=True), gate_proj, up_proj, down_proj
    )
    partial_out = partial_out.reshape(tp_count, expert_count * capacity, model_width)
    width_parts = lax.all_to_all(partial_out, "tp", split_axis=0, concat_axis=0, tiled=True)
    summed = jnp.sum(width_parts.astype(jnp.float32), 0).reshape(
        expert_count, capacity, model_width
    )
    returned = (
        lax.all_to_all(summed.astype(jnp.bfloat16), "sp", split_axis=0, concat_axis=0, tiled=True)
        .astype(summed.dtype)
        .reshape(expert_count * capacity, model_width)
    )
    picked = jnp.dot(
        select.astype(jnp.float32).T,
        returned,
        precision=lax.Precision.HIGHEST,
        preferred_element_type=jnp.float32,
    )
    routed = jnp.sum(picked.reshape(tok_rows, 2, model_width) * own_weights[..., None], 1)
    return (middle_f + routed).astype(jnp.bfloat16)


def solution(mesh):
    return jax.shard_map(
        per_device,
        mesh=mesh,
        in_specs=(
            P("sp", "tp"),
            P("sp", "tp"),
            P("sp", "tp"),
            P("tp"),
            P(("sp", "tp"), None),
            P("tp", None),
            P(),
            P("sp", None),
            P("sp", None),
            P("sp", None, "tp"),
            P("sp", None, "tp"),
            P("sp", "tp", None),
        ),
        out_specs=P(("sp", "tp"), None),
        check_vma=False,
    )
```

```python
import jax
import jax.numpy as jnp
import numpy as np
from jax import lax
from jax.experimental import pallas as pl
from jax.experimental.pallas import tpu as pltpu
from jax.sharding import PartitionSpec as P

HEAD = 64
WINDOW = 128


norm_epsilon = 1e-06


def from_behind(block, axis, distance):
    devices = range(lax.axis_size(axis))
    route = [(i - distance, i) for i in devices if i - distance in devices]
    return lax.ppermute(block, axis, route)


def rotary(values_in, positions, head_count):
    halfway = HEAD // 2
    frequency = 10000.0 ** (-jnp.arange(halfway, dtype=jnp.float32) * 2.0 / HEAD)
    angles = positions.astype(jnp.float32)[:, None] * frequency[None, :]
    cosine = jnp.cos(angles)[:, None, :]
    sine_part = jnp.sin(angles)[:, None, :]
    reshaped = values_in.astype(jnp.float32).reshape(values_in.shape[0], head_count, HEAD)
    front_part = reshaped[..., :halfway]
    back_part = reshaped[..., halfway:]
    turned = jnp.concatenate(
        [front_part * cosine - back_part * sine_part, back_part * cosine + front_part * sine_part],
        -1,
    )
    return turned.astype(jnp.bfloat16)


def attend(query_blocks, key_pairs, value_pairs, sink_grid, key_start):
    block_count = query_blocks.shape[0]
    window_len = query_blocks.shape[1]
    scores = jnp.einsum(
        "bqkgd,bskd->bkgqs", query_blocks, key_pairs, preferred_element_type=jnp.float32
    ) * HEAD ** (-0.5)
    row_idx = jnp.arange(window_len)[:, None]
    col_idx = jnp.arange(2 * window_len)[None, :]
    distance = row_idx - col_idx + window_len
    key_pos = key_start + jnp.arange(block_count)[:, None, None] * window_len + col_idx[None]
    allowed = (distance >= 0)[None] & (distance < window_len)[None] & (key_pos >= 0)
    scores = jnp.where(allowed[:, None, None], scores, -jnp.inf)
    sink_full = sink_grid[None, :, :, None]
    highest = jnp.maximum(jnp.max(scores, -1), sink_full)
    exp_scores = jnp.exp(scores - highest[..., None])
    denominator = jnp.sum(exp_scores, -1) + jnp.exp(sink_full - highest)
    weighted = jnp.einsum(
        "bkgqs,bskd->bkgqd",
        exp_scores.astype(jnp.bfloat16),
        value_pairs,
        preferred_element_type=jnp.float32,
    )
    normalized = weighted / denominator[..., None]
    return (
        jnp.transpose(normalized, (0, 3, 1, 2, 4))
        .astype(jnp.bfloat16)
        .reshape(block_count * window_len, -1)
    )


def slot_select(picks_in, expert_count, capacity):
    flattened = picks_in.reshape(-1)
    onehot = (flattened[:, None] == jnp.arange(expert_count, dtype=jnp.int32)[None, :]).astype(
        jnp.int32
    )
    rank_of = jnp.sum(jnp.cumsum(onehot, 0) * onehot, 1) - 1
    slot_of = flattened * capacity + rank_of
    chosen = jnp.arange(expert_count * capacity, dtype=jnp.int32)[:, None] == slot_of[None, :]
    return chosen.astype(jnp.bfloat16)


def expert_part(rows_in, gate_proj, up_proj, down_proj):
    in_shape = rows_in.shape
    flattened = rows_in.reshape(-1, in_shape[-1])
    gate_val = jnp.dot(flattened, gate_proj[0], preferred_element_type=jnp.float32)
    up_val = jnp.dot(flattened, up_proj[0], preferred_element_type=jnp.float32)
    hidden = (jax.nn.silu(gate_val) * up_val).astype(jnp.bfloat16)
    return (
        jnp.dot(hidden, down_proj[0], preferred_element_type=jnp.float32)
        .astype(jnp.bfloat16)
        .reshape(in_shape)
    )


GROUPS = 4
LANES = 128
MESH = pl.DeviceIdType.MESH
VIA, ON, DIAG = 0, 1, 2


PIECES = 2


def group_kernel(
    sink_hbm, q_hbm, k_hbm, v_hbm, row_hbm, base_hbm, resid_hbm, gain_hbm, ids_hbm, weights_hbm,
    wo_hbm, wg_hbm, wu_hbm, wd_hbm, out,
    sink, q_in, k_in, v_in, turn_row, turn_base, resid, gain, ids, weights, in_sem,
    wo, wg, wu, wd, w_sem,
    rim, rim_s, rim_r, asks, keys, vals, att,
    proj, rs_in, rs_s, rs_r,
    sel, ext,
    mid, normed, outb, rows,
    di_s, di_r, ag_s, ag_r, pt_s, pt_r,
    hid, outp, pr, pr_s, pr_r,
    comb, rs2, r2_s, r2_r,
    ret, back, bk_s, bk_r,
):
    sp = lax.axis_index("sp")
    t = lax.axis_index("tp")
    sp_n = lax.axis_size("sp")
    core = lax.rem(sp, 2)
    z = sp // 2
    tp_n, row_n, width = proj.shape
    cap = outb.shape[1]
    half = GROUPS * cap
    flip1 = t + 1 - 2 * lax.rem(t, 2)
    flip2 = lax.rem(t + 2, 4)
    flip3 = lax.rem(flip1 + 2, 4)
    peer = [t, flip1, flip2, flip3]
    via_t = flip1 + core * (flip2 - flip1)
    on_t = flip2 + core * (flip1 - flip2)
    partner = sp + 1 - 2 * core
    plane = [z, z + 1 - 2 * lax.rem(z, 2), lax.rem(z + 2, GROUPS), GROUPS - 1 - z]

    barrier = pltpu.get_barrier_semaphore()
    rim_peer = lax.rem(sp + 2 * core - 1 + sp_n, sp_n)
    friends = [(sp, peer[d]) for d in (1, 2, 3)]
    friends += [(plane[i] * 2 + core, t) for i in (1, 2, 3)] + [(partner, t), (rim_peer, t)]
    for dev in friends:
        pl.semaphore_signal(barrier, inc=1, device_id=dev, device_id_type=MESH)

    moves = (
        (row_hbm, turn_row), (base_hbm, turn_base), (q_hbm, q_in), (k_hbm, k_in), (v_hbm, v_in),
        (ids_hbm, ids), (weights_hbm, weights), (sink_hbm, sink),
        (resid_hbm, resid), (gain_hbm, gain),
    )
    feeds = [pltpu.make_async_copy(a, b, in_sem.at[i]) for i, (a, b) in enumerate(moves)]
    loads = [
        pltpu.make_async_copy(a, b, w_sem.at[i])
        for i, (a, b) in enumerate(((wo_hbm, wo), (wg_hbm, wg), (wu_hbm, wu), (wd_hbm, wd)))
    ]
    for c in feeds + loads:
        c.start()

    sent = []

    def describe(src, dst, ss, rs, dev):
        return pltpu.make_async_remote_copy(
            src_ref=src, dst_ref=dst, send_sem=ss, recv_sem=rs, device_id=dev, device_id_type=MESH
        )

    def send(src, dst, ss, rs, dev):
        c = describe(src, dst, ss, rs, dev)
        c.start()
        sent.append(c)
        return c

    bf = jnp.bfloat16
    f32 = jnp.float32
    local = q_in.shape[0]
    tiles = k_in.shape[1] // LANES
    pairs = q_in.shape[1] // LANES
    edge = WINDOW
    pad = keys.shape[1] - local - edge
    span = pad + edge + row_n

    for c in feeds[:-2]:
        c.wait()
    at_sp = lax.broadcasted_iota(jnp.int32, turn_base.shape, 0) == sp
    start = jnp.sum(jnp.where(at_sp, turn_base[...], 0.0), 0, keepdims=True)
    cb, sb = start[:, :LANES], start[:, LANES:]
    cr = turn_row[:, :LANES]
    sr = turn_row[:, LANES:]
    cosine = cb * cr - sb * sr
    sine = sb * cr + cb * sr
    spot = lax.broadcasted_iota(jnp.int32, (LANES, LANES), 0)
    lane_i = lax.broadcasted_iota(jnp.int32, (LANES, LANES), 1)
    swapped = jnp.where(lax.rem(lane_i, HEAD) < HEAD // 2, lane_i + HEAD // 2, lane_i - HEAD // 2)
    exchange = (spot == swapped).astype(bf)

    def turned(x, lo):
        n = x.shape[0]
        y = jnp.dot(x, exchange, preferred_element_type=f32)
        return x.astype(f32) * cosine[lo : lo + n] + y * sine[lo : lo + n]

    def doubled(x, ref, j, lo):
        n = x.shape[0]
        moved = pltpu.roll(x, HEAD, 1)
        first = lax.broadcasted_iota(jnp.int32, x.shape, 1) < HEAD
        ref[2 * j, lo : lo + n, :] = jnp.where(first, x, moved).astype(bf)
        ref[2 * j + 1, lo : lo + n, :] = jnp.where(first, moved, x).astype(bf)

    rim_next = lax.rem(sp + 1, sp_n)
    rims = [
        describe(
            src.at[pl.ds(local - edge, edge)], rim.at[i], rim_s.at[i], rim_r.at[i], (rim_next, t)
        )
        for i, src in enumerate((k_in, v_in))
    ]

    def rim_out():
        @pl.when(sp < sp_n - 1)
        def _():
            for c in rims:
                c.start()

    def fill(k_src, v_src, lo):
        for j in range(tiles):
            cols = slice(j * LANES, (j + 1) * LANES)
            doubled(turned(k_src[:, cols], lo), keys, j, lo + pad)
            doubled(v_src[:, cols].astype(f32), vals, j, lo + pad)

    def ask():
        lane = lax.broadcasted_iota(jnp.int32, (local, LANES), 1)
        for j in range(pairs):
            q = turned(q_in[:, j * LANES : (j + 1) * LANES], edge) * HEAD ** (-0.5)
            head = [jnp.where(lane < HEAD, q, 0.0), jnp.where(lane < HEAD, 0.0, q)]
            for i in (0, 1):
                for b in range(tp_n):
                    asks[b, j, i * row_n : (i + 1) * row_n, :] = head[i][
                        b * row_n : (b + 1) * row_n
                    ].astype(bf)
        keys[:, :pad, :] = jnp.zeros((keys.shape[0], pad, LANES), bf)
        vals[:, :pad, :] = jnp.zeros((keys.shape[0], pad, LANES), bf)

    def fill_own():
        fill(k_in, v_in, edge)

    upper = t >= tp_n // 2
    turn_order = [
        jnp.where(upper, t, flip3),
        jnp.where(upper, flip3, flip2),
        flip1,
        jnp.where(upper, flip2, t),
    ]

    def attend_block(i):
        b = turn_order[i]
        start_at = pl.multiple_of(b * row_n, row_n)
        shape = (2 * row_n, span)
        row = lax.rem(lax.broadcasted_iota(jnp.int32, shape, 0), row_n)
        col = lax.broadcasted_iota(jnp.int32, shape, 1)
        ahead = col - row
        key_pos = sp * local + b * row_n - pad - edge + col
        allowed = (ahead > pad + edge - WINDOW) & (ahead <= pad + edge) & (key_pos >= 0)
        lane = lax.broadcasted_iota(jnp.int32, (row_n, LANES), 1)
        top = lax.broadcasted_iota(jnp.int32, (2 * row_n, 1), 0) < row_n
        window = pl.ds(start_at, span)
        all_j = range(pairs)
        scores = [
            lax.dot_general(
                asks[b, j], keys[j, window, :], (((1,), (1,)), ((), ())),
                preferred_element_type=f32,
            )
            for j in all_j
        ]
        scores = [jnp.where(allowed, s, -jnp.inf) for s in scores]
        rest = [jnp.where(top, sink[2 * j], sink[2 * j + 1]) for j in all_j]
        highest = [
            jnp.maximum(jnp.max(scores[j], -1, keepdims=True), rest[j]) for j in all_j
        ]
        probs = [jnp.exp(scores[j] - highest[j]) for j in all_j]
        mixed = [
            jnp.dot(probs[j].astype(bf), vals[j, window, :], preferred_element_type=f32)
            for j in all_j
        ]
        share = [
            1.0 / (jnp.sum(probs[j], -1, keepdims=True) + jnp.exp(rest[j] - highest[j]))
            for j in all_j
        ]
        for j in all_j:
            m = mixed[j] * share[j]
            att[:, j * LANES : (j + 1) * LANES] = jnp.where(
                lane < HEAD, m[:row_n], m[row_n:]
            ).astype(bf)
        if i == 0:
            loads[0].wait()
        proj[b] = jnp.dot(att[...], wo[...], preferred_element_type=f32).astype(bf)

    lead = [via_t, on_t]

    def part(h):
        size = width // 2
        return slice(h * size, (h + 1) * size)

    def given(slot, h, b, to):
        return describe(
            proj.at[b, :, part(h)], rs_in.at[slot, :, part(h)],
            rs_s.at[slot, h], rs_r.at[slot, h], (sp, to),
        )

    def give(i):
        b = turn_order[i]
        slot = jnp.where(b == flip3, DIAG, VIA)
        for h in (0, 1):

            @pl.when((b == flip3) | (b == lead[h]))
            def _():
                given(slot, h, b, lead[h]).start()

    def give_on(h):
        given(DIAG, h, 0, lead[h]).wait_recv()
        b = lead[1 - h]
        proj[b, :, part(h)] = (
            proj[b, :, part(h)].astype(f32) + rs_in[DIAG, :, part(h)].astype(f32)
        ).astype(bf)
        c = given(ON, h, b, b)
        c.start()
        sent.append(c)

    def rim_in(now):
        @pl.when(now & (sp > 0))
        def _():
            for c in rims:
                c.wait_recv()

        @pl.when(now & (sp == 0))
        def _():
            rim[...] = jnp.zeros(rim.shape, bf)

        @pl.when(now)
        def _():
            fill(rim.at[0], rim.at[1], 0)

    def slots():
        def mine(x):
            x = jnp.broadcast_to(x, (8, x.shape[1]))
            x = jnp.where(t >= 2, x[:, LANES:], x[:, :LANES])
            return jnp.where(lax.rem(t, 2) == 1, pltpu.roll(x, row_n, 1), x)

        picks = [mine(ids[k : k + 1, :]) for k in (0, 1)]
        parts = [mine(weights[k : k + 1, :]) for k in (0, 1)]
        lane = lax.broadcasted_iota(jnp.int32, (8, LANES), 1)
        sub = lax.broadcasted_iota(jnp.int32, (8, LANES), 0)
        group = jnp.where(lane < row_n, picks[0] // 2, -1)
        hit = sub == group
        before = (spot < lane_i).astype(bf)
        rank = jnp.dot(hit.astype(f32).astype(bf), before, preferred_element_type=f32)
        rank = jnp.sum(jnp.where(hit, rank, 0.0), 0, keepdims=True).astype(jnp.int32)
        slot = group[0:1] * cap + rank
        slot = jnp.where(lane[0:1] < row_n, slot, -1)
        chosen = (spot == jnp.broadcast_to(slot, (LANES, LANES))).astype(f32).astype(bf)
        sel[0] = chosen
        sel[1] = lax.dot_general(
            (spot == lane_i).astype(f32).astype(bf), chosen, (((1,), (1,)), ((), ())),
            preferred_element_type=f32,
        ).astype(bf)
        table = jnp.zeros((8, LANES), f32)
        for p in (0, 1):
            w = sum(jnp.where(lax.rem(picks[k], 2) == p, parts[k], 0.0) for k in (0, 1))
            w = jnp.where(lane < row_n, w, 0.0)
            high = w.astype(bf).astype(f32)
            table = jnp.where(sub == p, high, table)
            table = jnp.where(sub == p + 2, w - high, table)
        table = jnp.concatenate([table, jnp.zeros((LANES - 8, LANES), f32)], 0).astype(bf)
        ext[...] = lax.dot_general(
            chosen, table, (((1,), (1,)), ((), ())), preferred_element_type=f32
        ).astype(bf)

    def meet():
        pl.semaphore_wait(barrier, len(friends))

    def gathered():
        for h in (0, 1):
            given(VIA, h, 0, lead[h]).wait_recv()
            given(ON, h, 0, lead[1 - h]).wait_recv()

    ask()
    fill_own()
    meet()
    rim_out()
    attend_block(0)
    give(0)
    rim_in(upper)
    attend_block(1)
    give(1)
    rim_in(t < tp_n // 2)
    attend_block(2)
    give(2)
    attend_block(3)
    give(3)
    slots()
    give_on(0)
    give_on(1)
    gathered()
    for c in feeds[-2:]:
        c.wait()
    total = resid[...].astype(f32) + (
        proj[t].astype(f32) + rs_in[VIA].astype(f32) + rs_in[ON].astype(f32)
    )
    middle = total.astype(bf)
    mid[...] = middle
    mf = middle.astype(f32)
    scale = lax.rsqrt(jnp.mean(mf * mf, -1, keepdims=True) + norm_epsilon)
    normed[...] = (mf * scale * gain[...]).astype(bf)

    def block(tt, cc, zz, g=None):
        first = pl.multiple_of((cc * tp_n + tt) * cap, cap)
        if g is None:
            return rows.at[zz, pl.ds(first, cap)]
        return rows.at[zz, pl.ds(pl.multiple_of(first + g * (cap // 2), cap // 2), cap // 2)]

    def pack(g, ref):
        spots = pl.ds(pl.multiple_of(g * cap, cap), cap)
        ref[:, :width] = jnp.dot(
            sel[0, spots, :row_n], normed[...], preferred_element_type=f32
        ).astype(bf)
        ref[:, width:] = ext[spots, :]

    ag = {}
    pt = {}
    swap = {}
    r2 = {}
    disp = {}
    bk = {}

    def push(step, g, half_i, i, tt, to):
        ref = block(tt, core, plane[i], half_i)
        n = 2 * step + g
        ag[(step, g, i)] = send(ref, ref, ag_s.at[n, i], ag_r.at[n, i], (sp, to))

    def across(d, i, tt):
        ref = block(tt, core, plane[i])
        pt[(d, i)] = send(ref, ref, pt_s.at[d, i], pt_r.at[d, i], (partner, t))

    def dispatch(i):
        g = plane[i]
        pack(g, outb.at[i])
        disp[i] = send(outb.at[i], block(t, core, z), di_s.at[i], di_r.at[i], (2 * g + core, t))

    def spread(i):
        if i:
            disp[i].wait_recv()
        for g in (0, 1):
            push(0, g, g, i, t, lead[g])
        for g in (0, 1):
            push(1, g, 1 - g, i, t, lead[g])
        across(3, i, t)

    def relay(i, g):
        ag[(0, g, i)].wait_recv()
        push(2, g, g, i, lead[g], lead[1 - g])

    def other(i):
        for g in (0, 1):
            ag[(1, g, i)].wait_recv()
            across(g, i, lead[g])

    def corner(i):
        for g in (0, 1):
            ag[(2, g, i)].wait_recv()
        across(2, i, flip3)

    def widen(i, h):
        if h == 0:
            for d in range(4):
                pt[(d, i)].wait_recv()
        if i == 0 and h == 0:
            for c in loads[1:]:
                c.wait()
        size = wg.shape[1] // PIECES
        cols = pl.ds(h * size, size)
        x = rows[plane[i], :, :width]
        g = jnp.dot(x, wg[:, cols], preferred_element_type=jnp.float32)
        u = jnp.dot(x, wu[:, cols], preferred_element_type=jnp.float32)
        hid[i, :, cols] = (g / (1.0 + jnp.exp(-g)) * u).astype(jnp.bfloat16)

    def part_cols(i, h):
        size = width // PIECES
        return pl.ds(h * size, size)

    def narrow(i, h):
        ext = rows[plane[i], :, width:].astype(jnp.float32)
        lane = lax.broadcasted_iota(jnp.int32, ext.shape, 1)
        mine = (lane == core) | (lane == core + 2)
        weight = jnp.sum(jnp.where(mine, ext, 0.0), -1, keepdims=True)
        cols = part_cols(i, h)
        y = jnp.dot(hid[i], wd[:, cols], preferred_element_type=jnp.float32)
        outp[i, :, cols] = (y * weight).astype(jnp.bfloat16)

        here = part_cols(i, h)
        other_half = outp.at[i, pl.ds(pl.multiple_of((1 - core) * half, half), half), here]
        swap[(i, h)] = send(
            other_half, pr.at[i, :, here], pr_s.at[i, h], pr_r.at[i, h], (partner, t)
        )

    def own(i, h, tt):
        here = part_cols(i, h)
        mine = pl.ds(pl.multiple_of((core * tp_n + tt) * cap, cap), cap)
        theirs = pl.ds(pl.multiple_of(tt * cap, cap), cap)
        return outp[i, mine, here].astype(jnp.float32) + pr[i, theirs, here].astype(jnp.float32)

    def ship(d, i, h, to):
        here = part_cols(i, h)
        r2[(d, i, h)] = send(
            comb.at[i, d, :, here], rs2.at[i, d, :, here],
            r2_s.at[d, i, h], r2_r.at[d, i, h], (sp, to),
        )

    def combine(i, h):
        here = part_cols(i, h)
        swap[(i, h)].wait_recv()
        comb[i, DIAG, :, here] = own(i, h, flip3).astype(jnp.bfloat16)
        ship(DIAG, i, h, lead[h])
        comb[i, VIA, :, here] = own(i, h, lead[h]).astype(jnp.bfloat16)
        ship(VIA, i, h, lead[h])

    def combine_on(i, h):
        here = part_cols(i, h)
        r2[(DIAG, i, h)].wait_recv()
        comb[i, ON, :, here] = (
            own(i, h, lead[1 - h]) + rs2[i, DIAG, :, here].astype(jnp.float32)
        ).astype(jnp.bfloat16)
        ship(ON, i, h, lead[1 - h])

    def finish(i, h):
        here = part_cols(i, h)
        acc = own(i, h, t)
        for d in (VIA, ON):
            r2[(d, i, h)].wait_recv()
            acc = acc + rs2[i, d, :, here].astype(jnp.float32)
        if i:
            ret[i, :, here] = acc.astype(jnp.bfloat16)
            bk[(i, h)] = describe(
                ret.at[i, :, here], back.at[z, :, here], bk_s.at[i, h], bk_r.at[i, h],
                (2 * plane[i] + core, t),
            )
            bk[(i, h)].start()
        else:
            back[z, :, here] = acc.astype(jnp.bfloat16)

    pack(z, block(t, core, z))
    spread(0)
    dispatch(1)
    dispatch(2)
    relay(0, 0)
    dispatch(3)
    relay(0, 1)
    spread(1)
    other(0)
    corner(0)
    relay(1, 0)
    relay(1, 1)
    spread(2)
    widen(0, 0)
    widen(0, 1)
    corner(1)
    other(1)
    relay(2, 0)
    relay(2, 1)
    spread(3)
    narrow(0, 0)
    widen(1, 0)
    other(2)
    widen(1, 1)
    combine(0, 0)
    corner(2)
    narrow(1, 0)
    relay(3, 0)
    relay(3, 1)
    widen(2, 0)
    widen(2, 1)
    combine(1, 0)
    narrow(2, 0)
    other(3)
    narrow(2, 1)
    corner(3)
    combine(2, 0)
    combine_on(1, 0)
    combine(2, 1)
    widen(3, 0)
    widen(3, 1)
    combine_on(2, 0)
    narrow(3, 0)
    narrow(3, 1)
    combine_on(2, 1)
    finish(1, 0)
    combine(3, 0)
    finish(2, 0)
    combine(3, 1)
    finish(2, 1)
    combine_on(3, 0)
    narrow(1, 1)
    combine(1, 1)
    combine_on(3, 1)
    finish(3, 0)
    narrow(0, 1)
    combine(0, 1)
    combine_on(1, 1)
    combine_on(0, 0)
    finish(3, 1)
    combine_on(0, 1)
    finish(1, 1)
    finish(0, 0)
    finish(0, 1)
    for c in sent:
        c.wait_send()
    for h in (0, 1):
        for slot in (VIA, DIAG):
            given(slot, h, 0, lead[h]).wait_send()

    @pl.when(sp < sp_n - 1)
    def _():
        for c in rims:
            c.wait_send()

    for h in range(PIECES):
        here = part_cols(0, h)
        for i in range(1, GROUPS):
            bk[(i, h)].wait_recv()
        routed = jnp.dot(
            sel[1, :row_n, :],
            back[:, :, here].reshape(half, width // PIECES),
            preferred_element_type=f32,
        )
        out[:, here] = mid[:, here].astype(f32) + routed
    for c in bk.values():
        c.wait_send()


def group_layer(
    queries, key_rows, values, sink_logits, residual, out_weight, norm_gain, expert_ids,
    route_weight, gate, up, down,
):
    row_n, width = residual.shape
    local = queries.shape[0]
    tp_n = lax.axis_size("tp")
    expert_n = lax.axis_size("sp")
    cap = 2 * max(1, 2 * row_n // expert_n)
    ext_width = width + LANES
    ff = gate.shape[-1]
    half = GROUPS * cap
    kv_heads = key_rows.shape[1] // HEAD
    frequency = 10000.0 ** (-(np.arange(LANES) % (HEAD // 2)) * 2.0 / HEAD)
    sign = np.where(np.arange(LANES) % HEAD < HEAD // 2, -1.0, 1.0)

    def turns(positions):
        angle = positions[:, None] * frequency[None, :]
        return jnp.asarray(
            np.concatenate([np.cos(angle), np.sin(angle) * sign], 1), jnp.float32
        )

    turn_row = turns(np.arange(local + WINDOW) - float(WINDOW))
    turn_base = turns(np.arange(expert_n) * float(local))
    bf = jnp.bfloat16
    dma = pltpu.SemaphoreType.DMA
    vmem = pl.BlockSpec(memory_space=pltpu.VMEM)
    hbm = pl.BlockSpec(memory_space=pltpu.HBM)
    total = pl.pallas_call(
        group_kernel,
        out_shape=jax.ShapeDtypeStruct((row_n, width), jnp.float32),
        in_specs=[hbm] * 14,
        out_specs=vmem,
        scratch_shapes=[
            pltpu.SMEM(sink_logits.shape, jnp.float32),
            pltpu.VMEM(queries.shape, bf),
            pltpu.VMEM(key_rows.shape, bf),
            pltpu.VMEM(values.shape, bf),
            pltpu.VMEM(turn_row.shape, jnp.float32),
            pltpu.VMEM(turn_base.shape, jnp.float32),
            pltpu.VMEM(residual.shape, bf),
            pltpu.VMEM((1, width), jnp.float32),
            pltpu.VMEM(expert_ids.shape[::-1], jnp.int32),
            pltpu.VMEM(route_weight.shape[::-1], jnp.float32),
            dma((10,)),
            pltpu.VMEM(out_weight.shape, bf),
            pltpu.VMEM((width, ff), bf),
            pltpu.VMEM((width, ff), bf),
            pltpu.VMEM((ff, width), bf),
            dma((4,)),
            pltpu.VMEM((2, WINDOW, key_rows.shape[1]), bf),
            dma((2,)),
            dma((2,)),
            pltpu.VMEM((tp_n, queries.shape[1] // LANES, 2 * row_n, LANES), bf),
            pltpu.VMEM((kv_heads, local + WINDOW + row_n, LANES), bf),
            pltpu.VMEM((kv_heads, local + WINDOW + row_n, LANES), bf),
            pltpu.VMEM((row_n, queries.shape[1]), bf),
            pltpu.VMEM((tp_n, row_n, width), bf),
            pltpu.VMEM((3, row_n, width), bf),
            dma((3, 2)),
            dma((3, 2)),
            pltpu.VMEM((2, LANES, LANES), bf),
            pltpu.VMEM((LANES, LANES), bf),
            pltpu.VMEM((row_n, width), bf),
            pltpu.VMEM((row_n, width), bf),
            pltpu.VMEM((GROUPS, cap, ext_width), bf),
            pltpu.VMEM((GROUPS, 2 * half, ext_width), bf),
            dma((GROUPS,)),
            dma((GROUPS,)),
            dma((6, GROUPS)),
            dma((6, GROUPS)),
            dma((4, GROUPS)),
            dma((4, GROUPS)),
            pltpu.VMEM((GROUPS, 2 * half, ff), bf),
            pltpu.VMEM((GROUPS, 2 * half, width), bf),
            pltpu.VMEM((GROUPS, half, width), bf),
            dma((GROUPS, 2)),
            dma((GROUPS, 2)),
            pltpu.VMEM((GROUPS, 3, cap, width), bf),
            pltpu.VMEM((GROUPS, 3, cap, width), bf),
            dma((3, GROUPS, 2)),
            dma((3, GROUPS, 2)),
            pltpu.VMEM((GROUPS, cap, width), bf),
            pltpu.VMEM((GROUPS, cap, width), bf),
            dma((GROUPS, 2)),
            dma((GROUPS, 2)),
        ],
        compiler_params=pltpu.CompilerParams(
            collective_id=0, has_side_effects=True, vmem_limit_bytes=50 * 2**20
        ),
    )(
        *(
            pltpu.with_memory_space_constraint(x, pltpu.HBM)
            for x in (
                sink_logits, queries, key_rows, values, turn_row, turn_base, residual,
                norm_gain[None], expert_ids.T, route_weight.T, out_weight, gate[0], up[0], down[0],
            )
        )
    )
    return total.astype(bf)


def per_device(
    queries,
    key_rows,
    values,
    sink_logits,
    residual,
    out_weight,
    norm_gain,
    expert_ids,
    route_weight,
    gate_proj,
    up_proj,
    down_proj,
):
    local_len = queries.shape[0]
    if lax.axis_size("tp") == 4 and lax.axis_size("sp") == 2 * GROUPS:
        return group_layer(
            queries, key_rows, values, sink_logits, residual, out_weight, norm_gain,
            expert_ids, route_weight, gate_proj, up_proj, down_proj,
        )
    q_heads = sink_logits.shape[0]
    kv_heads = key_rows.shape[1] // HEAD
    group_size = q_heads // kv_heads
    window_len = WINDOW
    seq_start = lax.axis_index("sp") * local_len
    rim_pair = jnp.stack([key_rows[local_len - window_len :], values[local_len - window_len :]])
    rim_pair = from_behind(rim_pair, "sp", 1)
    key_ext = jnp.concatenate([rim_pair[0], key_rows], 0)
    val_ext = jnp.concatenate([rim_pair[1], values], 0)
    positions = seq_start + jnp.arange(local_len, dtype=jnp.int32)
    ext_positions = seq_start - window_len + jnp.arange(local_len + window_len, dtype=jnp.int32)
    rot_query = rotary(queries, positions, q_heads)
    rot_key = rotary(key_ext, ext_positions, kv_heads)
    block_count = local_len // window_len
    query_blocks = rot_query.reshape(block_count, window_len, kv_heads, group_size, HEAD)
    key_blocks = rot_key.reshape(block_count + 1, window_len, kv_heads, HEAD)
    value_blocks = val_ext.reshape(block_count + 1, window_len, kv_heads, HEAD)
    key_pairs = jnp.concatenate([key_blocks[:-1], key_blocks[1:]], 1)
    value_pairs = jnp.concatenate([value_blocks[:-1], value_blocks[1:]], 1)
    sink_grid = sink_logits.reshape(kv_heads, group_size)
    attended = attend(query_blocks, key_pairs, value_pairs, sink_grid, seq_start - window_len)
    tok_rows = residual.shape[0]
    tp_count = lax.axis_size("tp")
    tp_index = lax.axis_index("tp")
    projected = lax.psum_scatter(
        jnp.dot(attended, out_weight, preferred_element_type=jnp.float32).astype(jnp.bfloat16),
        "tp",
        scatter_dimension=0,
        tiled=True,
    ).astype(jnp.float32)
    middle = (residual.astype(jnp.float32) + projected).astype(jnp.bfloat16)
    middle_f = middle.astype(jnp.float32)
    normed = (
        middle_f
        * lax.rsqrt(jnp.mean(middle_f * middle_f, -1, keepdims=True) + norm_epsilon)
        * norm_gain
    ).astype(jnp.bfloat16)
    expert_count = lax.axis_size("sp")
    capacity = 2 * max(1, 2 * tok_rows // expert_count)
    model_width = normed.shape[1]
    own_ids = lax.dynamic_slice_in_dim(expert_ids, tp_index * tok_rows, tok_rows, 0)
    own_weights = lax.dynamic_slice_in_dim(route_weight, tp_index * tok_rows, tok_rows, 0)
    select = slot_select(own_ids, expert_count, capacity)
    token_select = jnp.sum(select.reshape(expert_count * capacity, tok_rows, 2), -1)
    outbound = jnp.dot(token_select, normed, preferred_element_type=jnp.float32).astype(
        jnp.bfloat16
    )
    outbound = outbound.reshape(expert_count, capacity, model_width)
    arrived = lax.all_to_all(outbound, "sp", split_axis=0, concat_axis=0, tiled=True)
    partial_out = expert_part(
        lax.all_gather(arrived, "tp", axis=0, tiled=True), gate_proj, up_proj, down_proj
    )
    partial_out = partial_out.reshape(tp_count, expert_count * capacity, model_width)
    width_parts = lax.all_to_all(partial_out, "tp", split_axis=0, concat_axis=0, tiled=True)
    summed = jnp.sum(width_parts.astype(jnp.float32), 0).reshape(
        expert_count, capacity, model_width
    )
    returned = (
        lax.all_to_all(summed.astype(jnp.bfloat16), "sp", split_axis=0, concat_axis=0, tiled=True)
        .astype(summed.dtype)
        .reshape(expert_count * capacity, model_width)
    )
    picked = jnp.dot(
        select.astype(jnp.float32).T,
        returned,
        precision=lax.Precision.HIGHEST,
        preferred_element_type=jnp.float32,
    )
    routed = jnp.sum(picked.reshape(tok_rows, 2, model_width) * own_weights[..., None], 1)
    return (middle_f + routed).astype(jnp.bfloat16)


def solution(mesh):
    return jax.shard_map(
        per_device,
        mesh=mesh,
        in_specs=(
            P("sp", "tp"),
            P("sp", "tp"),
            P("sp", "tp"),
            P("tp"),
            P(("sp", "tp"), None),
            P("tp", None),
            P(),
            P("sp", None),
            P("sp", None),
            P("sp", None, "tp"),
            P("sp", None, "tp"),
            P("sp", "tp", None),
        ),
        out_specs=P(("sp", "tp"), None),
        check_vma=False,
    )
```
